128 devices in a mesh: sp: 64 (over z, y, x), tp: 2 (over core).
Axes of the slice: x: 4, y: 4, z: 4, core: 2. Of those that a mesh axis runs over, the one named last changes fastest.
Arguments:
- conv_out: bfloat16 [8192, 2048], P('sp', 'tp'), may hold values from -1500 to 1500
- ln_gain: float32 [2048], P('tp'), may hold values from 0.1 to 1.9
- taps: bfloat16 [31, 2048], P(None, 'tp'), may hold values from -1 to 1
- proj_weight: bfloat16 [2048, 2048], P('sp', 'tp'), may hold values from -0.125 to 0.125
- stream_mid: bfloat16 [8192, 2048], P('sp', 'tp'), may hold values from -6 to 6
- out_grad: bfloat16 [8192, 2048], P('sp', 'tp'), may hold values from -16 to 16
- routes: int32 [8192, 2], P('sp'), may hold values from 0 to 31, all different within a row; in each aligned block of 128 rows (0 to 127, 128 to 255, ...) at most 12 rows name the same one
- route_probs: float32 [8192, 2], P('sp'), may hold values from 0.2 to 1
- gate_slabs: bfloat16 [64, 2048, 1792], P('sp', None, 'tp'), may hold values from -0.125 to 0.125
- up_slabs: bfloat16 [64, 2048, 1792], P('sp', None, 'tp'), may hold values from -0.125 to 0.125
- down_slabs: bfloat16 [64, 1792, 2048], P('sp', 'tp'), may hold values from -0.09375 to 0.09375
Outputs:
- grad_input: bfloat16 [8192, 2048], P('sp', 'tp')
- grad_proj: float32 [2048, 2048], P('sp', 'tp')
- grad_gate: bfloat16 [64, 2048, 1792], P('sp', None, 'tp')
- grad_up: bfloat16 [64, 2048, 1792], P('sp', None, 'tp')
- grad_down: bfloat16 [64, 1792, 2048], P('sp', 'tp')
The draws below stay inside these ranges and needn't reach their ends.
Inputs may be any that keep to these rules, and one draw needn't show every extreme that they name: `routes`: each row names two different experts. Among the rows of one device no expert is named more than 12 times, and in every draw some device's rows name some expert exactly 12 times.
All inputs are finite; a program needn't handle non-finite values.
Results may differ from the reference program's by a relative error of at most 0.015.
Values may be sent and summed in bfloat16 or wider, within the bound.
A program may use at most 128 MiB of HBM per device.

```python
import math
import jax
import jax.numpy as jnp
import numpy as np
from jax import lax

D = 2048
EXP_HIDDEN = 3584
CONV_WIDTH = 31
TOK_DEV = 128
EXPERTS = 32
CAP = 12
TOKENS = 8192
N_SP = 64
N_TP = 2


def draw_conv_out(key, part):
    keys = jax.random.split(key, 3)
    columns = jnp.arange(D, dtype=jnp.float32)
    col_scale = jnp.exp(jax.random.uniform(keys[0], (D,), jnp.float32, 0.0, math.log(10.0))) * 3.0 ** (columns / D)
    row_scale = jnp.exp(jax.random.uniform(keys[1], (TOKENS, 1), jnp.float32, 0.0, math.log(10.0)))
    base = jnp.clip(jax.random.normal(keys[2], (TOKENS, D), jnp.float32), -5.0, 5.0)
    return (base * col_scale[None, :] * row_scale).astype(jnp.bfloat16)


def with_spikes(array, stream_key, source, target, parts, factor):
    owner, partner = [(jnp.arange(array.shape[axis_at]) // (array.shape[axis_at] // parts)).reshape([-1 if axis == axis_at else 1 for axis in range(array.ndim)]) for axis_at in (source, target)]
    chosen = jax.random.permutation(stream_key, parts)[partner]
    strong = (owner == chosen) | (owner == (partner + parts // 2) % parts)
    return jnp.where(strong, factor * array, array)


def steps_of(key, shape, shards, low, top_value):
    def one(dim, parts):
        draws = jax.random.uniform(jax.random.fold_in(jax.random.fold_in(key, 6), dim), (parts,), jnp.float32, low / len(shards), top_value / len(shards))
        return jnp.repeat(jnp.exp(draws), shape[dim] // parts).reshape((-1,) + (1,) * (len(shape) - dim - 1))

    loudness = one(*shards[0])
    for cut in shards[1:]:
        loudness = loudness * one(*cut)
    return loudness


def shared_out(own_key, own, number, rows, amount, top, most, skew):
    sequence = jax.random.permutation(own_key, amount)
    crowded, common = load_shares(amount, rows * top, most, skew, True), load_shares(amount, rows * top, most, skew, False)
    places = jnp.arange(amount)

    def named(tallies, offset_by):
        used = int((tallies > 0).sum())
        fixed = max(1, used // 4)
        passed = fixed + (places - fixed + offset_by * (used - fixed)) % max(1, amount - fixed)
        return jnp.zeros((amount,), jnp.int32).at[sequence[jnp.where(places < fixed, places, passed)]].set(jnp.asarray(tallies, jnp.int32))

    tallies = jnp.where(number % 4 == 0, named(crowded, number // 4), named(common, number - number // 4 - 1))
    mixed = jax.random.permutation(jax.random.fold_in(own, 3), amount)
    source_of, receiver = mixed[0:amount // 2 * 2:2], mixed[1:amount // 2 * 2:2]
    margin = jnp.minimum(tallies[source_of] - 1, most - tallies[receiver]) // 2
    margin = jnp.where((source_of == sequence[0]) | (receiver == sequence[0]) | (tallies[receiver] == 0), 0, jnp.maximum(margin, 0))
    passed = jax.random.randint(jax.random.fold_in(own, 4), (amount // 2,), 0, 1 << 20) % (margin + 1)
    tallies = tallies.at[source_of].add(-passed).at[receiver].add(passed)
    items = jnp.searchsorted(jnp.cumsum(tallies), jnp.arange(rows * top), side="right").astype(jnp.int32)
    table = items.reshape(top, rows).T
    table = table[jax.random.permutation(jax.random.fold_in(own, 1), rows)]
    offset_by = jax.random.randint(jax.random.fold_in(own, 2), (rows, 1), 0, top)
    return jnp.take_along_axis(table, (jnp.arange(top)[None, :] + offset_by) % top, axis=1)


def load_shares(count, total, bound, skew, full):
    weights = [(1 << 20) // math.isqrt(grade ** skew) + 1 for grade in range(1, count + 1)]
    largest = bound if full else min(bound, max(-(-total // count), total * weights[0] // sum(weights)))
    least = 1 if total - largest >= count - 1 else 0
    given, rest = [largest] + [least] * (count - 1), total - largest - least * (count - 1)
    while rest > 0:
        free = [i for i in range(1, count) if given[i] < largest] or [i for i in range(1, count) if given[i] < bound]
        pool, left = sum([weights[i] for i in free]), rest
        for i in free:
            more = min(bound - given[i], max(1, left * weights[i] // pool), rest)
            given[i] = given[i] + more
            rest = rest - more
    return np.array(given)


def scatter_about(key, extent, deviation, most, pieces=(), kind=jnp.bfloat16):
    array = deviation * jax.random.normal(key, extent, jnp.float32)
    if pieces:
        array = array * steps_of(key, extent, pieces, -0.22, 0.18)
    return jnp.clip(array, -most, most).astype(kind)


def gaussian_with(key, shape, width, most, shards, heavy, kind=jnp.bfloat16):
    values = width * jax.random.normal(key, shape, jnp.float32)
    if shards:
        values = values * steps_of(key, shape, shards, -0.22, 0.18)
    return jnp.clip(with_spikes(values, jax.random.fold_in(key, 3), *heavy), -most, most).astype(kind)


def setup_inputs(seed: int = 0) -> dict:
    splits = jax.random.split(jax.random.key(seed), 12)
    conv_out = draw_conv_out(jax.random.fold_in(splits[11], 71), 0)
    ln_gain = jnp.clip(1.0 + 0.18 * jax.random.normal(splits[1], (D,), jnp.float32), 0.1, 1.9)
    taps = scatter_about(splits[2], (CONV_WIDTH, D), CONV_WIDTH ** -0.5, 1.0, ((1, 2),))
    proj_weight = scatter_about(splits[3], (D, D), D ** -0.5, 0.125, ((0, 64), (1, 2)))
    stream_mid = scatter_about(splits[4], (TOKENS, D), 1.0, 6.0, ((0, 64), (1, 2)))
    out_grad = gaussian_with(splits[5], (TOKENS, D), 1.0, 16.0, ((0, 64), (1, 2)), (0, 1, 64, 4.0))
    routes_keys = jax.random.split(jax.random.fold_in(splits[6], 1), TOKENS // TOK_DEV)
    routes_turns = jax.random.permutation(jax.random.fold_in(splits[6], 3), TOKENS // TOK_DEV)
    routes = jax.vmap(lambda own, number: shared_out(jax.random.fold_in(splits[6], 2), own, number, TOK_DEV, EXPERTS, 2, CAP, 1))(routes_keys, routes_turns).reshape((TOKENS, 2))
    route_probs = jnp.clip(0.2 + 0.8 * jax.random.uniform(splits[7], (TOKENS, 2), jnp.float32) ** steps_of(splits[7], (TOKENS, 2), ((0, 64),), -0.2, 0.2), 0.2, 1.0)
    gate_slabs = scatter_about(splits[8], (2 * EXPERTS, D, EXP_HIDDEN // 2), D ** -0.5, 0.125, ((0, 64), (2, 2)))
    up_slabs = scatter_about(splits[9], (2 * EXPERTS, D, EXP_HIDDEN // 2), D ** -0.5, 0.125, ((0, 64), (2, 2)))
    down_slabs = scatter_about(splits[10], (2 * EXPERTS, EXP_HIDDEN // 2, D), EXP_HIDDEN ** -0.5, 0.09375, ((0, 64), (1, 2)))
    return {"conv_out": conv_out, "ln_gain": ln_gain, "taps": taps, "proj_weight": proj_weight, "stream_mid": stream_mid, "out_grad": out_grad, "routes": routes, "route_probs": route_probs, "gate_slabs": gate_slabs, "up_slabs": up_slabs, "down_slabs": down_slabs}


def dispatch_table(route_block, experts, capacity):
    tok_rows = route_block.shape[0]
    labels = jnp.arange(experts, dtype=jnp.int32)
    onehot = (route_block[:, :, None] == labels[None, None, :]).astype(jnp.float32)
    per_token = lax.optimization_barrier(jnp.sum(onehot, axis=1))
    earlier = (jnp.arange(tok_rows)[:, None] > jnp.arange(tok_rows)[None, :]).astype(jnp.float32)
    before = jnp.dot(earlier, per_token, precision=lax.Precision.HIGHEST)
    slot_index = lax.optimization_barrier(jnp.sum(onehot * before[:, None, :], axis=2)).astype(jnp.int32)
    position = route_block * capacity + slot_index
    columns = jnp.arange(experts * capacity, dtype=jnp.int32)
    first_pick = position[:, 0:1] == columns[None, :]
    second_pick = position[:, 1:2] == columns[None, :]
    return (first_pick, second_pick)

def half_grads(expert_in, expert_grad, weight, w_gate, w_up, w_down):
    gate_value = jnp.dot(expert_in, w_gate, preferred_element_type=jnp.float32)
    up_value = jnp.dot(expert_in, w_up, preferred_element_type=jnp.float32)
    gate_sig = jax.nn.sigmoid(gate_value)
    hidden_act = gate_value * gate_sig * up_value
    scaled = (weight[:, None] * hidden_act).astype(jnp.bfloat16)
    grad_down = jnp.dot(scaled.T, expert_grad, preferred_element_type=jnp.float32).astype(jnp.bfloat16)
    grad_hidden = weight[:, None] * jnp.dot(expert_grad, w_down.T, preferred_element_type=jnp.float32)
    grad_gate_pre = (grad_hidden * up_value * gate_sig * (1.0 + gate_value * (1.0 - gate_sig))).astype(jnp.bfloat16)
    grad_up_pre = (grad_hidden * gate_value * gate_sig).astype(jnp.bfloat16)
    grad_gate = jnp.dot(expert_in.T, grad_gate_pre, preferred_element_type=jnp.float32).astype(jnp.bfloat16)
    grad_up = jnp.dot(expert_in.T, grad_up_pre, preferred_element_type=jnp.float32).astype(jnp.bfloat16)
    quarter = w_gate.shape[1] // N_TP
    returned = jnp.zeros(expert_in.shape, jnp.float32)
    for core_index in range(N_TP):
        low_col = core_index * quarter
        high_col = low_col + quarter
        piece = jnp.dot(grad_gate_pre[:, low_col:high_col], w_gate[:, low_col:high_col].T, preferred_element_type=jnp.float32)
        piece = piece + jnp.dot(grad_up_pre[:, low_col:high_col], w_up[:, low_col:high_col].T, preferred_element_type=jnp.float32)
        rounded = lax.optimization_barrier(piece.astype(jnp.bfloat16))
        returned = returned + rounded.astype(jnp.float32)
    return (grad_gate, grad_up, grad_down, returned.astype(jnp.bfloat16))

def reference(conv_out, ln_gain, taps, proj_weight, stream_mid, out_grad, routes, route_probs, gate_slabs, up_slabs, down_slabs):
    slot_count = EXPERTS * CAP
    half_width = EXP_HIDDEN // 2

    def pack(inputs):
        route_block, mid_block, grad_block, prob_block = inputs
        first_pick, second_pick = dispatch_table(route_block, EXPERTS, CAP)
        route_table = (first_pick | second_pick).astype(jnp.float32)
        mid_slots = jnp.dot(route_table.T, mid_block.astype(jnp.float32), precision=lax.Precision.HIGHEST).astype(jnp.bfloat16)
        grad_slots = jnp.dot(route_table.T, grad_block.astype(jnp.float32), precision=lax.Precision.HIGHEST).astype(jnp.bfloat16)
        prob_slots = lax.optimization_barrier(jnp.sum(first_pick.astype(jnp.float32) * prob_block[:, 0:1] + second_pick.astype(jnp.float32) * prob_block[:, 1:2], axis=0))
        return (mid_slots, grad_slots, prob_slots)
    mid_slots, grad_slots, prob_slots = lax.map(pack, (routes.reshape(N_SP, TOK_DEV, 2), stream_mid.reshape(N_SP, TOK_DEV, D), out_grad.reshape(N_SP, TOK_DEV, D), route_probs.reshape(N_SP, TOK_DEV, 2)))

    def by_expert(slots):
        return slots.reshape(N_SP, EXPERTS, CAP, D).transpose(1, 0, 2, 3).reshape(EXPERTS, N_SP * CAP, D)
    probs_expert = prob_slots.reshape(N_SP, EXPERTS, CAP).transpose(1, 0, 2).reshape(EXPERTS, N_SP * CAP)

    def expert(inputs):
        expert_in, expert_grad, weight, gates, ups, downs = inputs
        first_half = half_grads(expert_in, expert_grad, weight, gates[0], ups[0], downs[0])
        second_half = half_grads(expert_in, expert_grad, weight, gates[1], ups[1], downs[1])
        return (jnp.stack([first_half[0], second_half[0]]), jnp.stack([first_half[1], second_half[1]]), jnp.stack([first_half[2], second_half[2]]), jnp.stack([first_half[3], second_half[3]]))
    grad_gate, grad_up, grad_down, returned = lax.map(expert, (by_expert(mid_slots), by_expert(grad_slots), probs_expert, gate_slabs.reshape(EXPERTS, 2, D, half_width), up_slabs.reshape(EXPERTS, 2, D, half_width), down_slabs.reshape(EXPERTS, 2, half_width, D)))
    returned = returned.reshape(EXPERTS, 2, N_SP, CAP, D).transpose(2, 0, 1, 3, 4)

    def unpack(inputs):
        route_block, back_rows, grad_block = inputs
        first_pick, second_pick = dispatch_table(route_block, EXPERTS, CAP)
        route_table = (first_pick | second_pick).astype(jnp.bfloat16)
        contrib = jnp.dot(route_table, back_rows[:, 0].reshape(slot_count, D), preferred_element_type=jnp.float32)
        contrib = contrib + jnp.dot(route_table, back_rows[:, 1].reshape(slot_count, D), preferred_element_type=jnp.float32)
        return (grad_block.astype(jnp.float32) + contrib).astype(jnp.bfloat16)
    grad_stream = lax.map(unpack, (routes.reshape(N_SP, TOK_DEV, 2), returned, out_grad.reshape(N_SP, TOK_DEV, D))).reshape(TOKENS, D)
    values = conv_out.astype(jnp.float32)
    row_mean = lax.optimization_barrier(jnp.mean(values, axis=1, keepdims=True))
    row_var = lax.optimization_barrier(jnp.mean(values * values, axis=1, keepdims=True)) - row_mean * row_mean
    inv_std = lax.rsqrt(row_var + 1e-06)
    normed = (values - row_mean) * inv_std
    scaled_z = normed * ln_gain[None, :]
    z_sig = jax.nn.sigmoid(scaled_z)
    activated = (scaled_z * z_sig).astype(jnp.bfloat16)
    grad_act = jnp.dot(grad_stream, proj_weight, preferred_element_type=jnp.float32)
    grad_normed = grad_act * z_sig * (1.0 + scaled_z * (1.0 - z_sig)) * ln_gain[None, :]
    first_mean = lax.optimization_barrier(jnp.mean(grad_normed, axis=1, keepdims=True))
    second_mean = lax.optimization_barrier(jnp.mean(grad_normed * normed, axis=1, keepdims=True))
    grad_conv = (inv_std * (grad_normed - first_mean - normed * second_mean)).astype(jnp.bfloat16)
    extended = jnp.concatenate([grad_conv, jnp.zeros((CONV_WIDTH - 1, D), jnp.bfloat16)], axis=0).astype(jnp.float32)
    tap_values = taps.astype(jnp.float32)
    grad_input = jnp.zeros((TOKENS, D), jnp.float32)
    for offset in range(CONV_WIDTH):
        grad_input = grad_input + tap_values[offset][None, :] * extended[offset:offset + TOKENS]
    grad_proj = jnp.dot(grad_stream.T, activated, preferred_element_type=jnp.float32)
    return (grad_input.astype(jnp.bfloat16), grad_proj, grad_gate.reshape(2 * EXPERTS, D, half_width), grad_up.reshape(2 * EXPERTS, D, half_width), grad_down.reshape(2 * EXPERTS, half_width, D))
```

```python
import functools

import jax
import jax.numpy as jnp
from jax import lax
from jax.experimental import pallas as pl
from jax.experimental.pallas import tpu as pltpu
from jax.sharding import PartitionSpec as P

D = 2048
HALF = 1024
MAIN = 8
REM = 4
MESH = pl.DeviceIdType.MESH
F32 = jnp.float32
BF16 = jnp.bfloat16


def nt(a, b):
    return lax.dot_general(a, b, (((1,), (1,)), ((), ())), preferred_element_type=F32)


def nn(a, b):
    return lax.dot_general(a, b, (((1,), (0,)), ((), ())), preferred_element_type=F32)


def tn(a, b):
    return lax.dot_general(a, b, (((0,), (0,)), ((), ())), preferred_element_type=F32)


def sp_copy(src, dst, send, recv, sp):
    return pltpu.make_async_remote_copy(
        src_ref=src, dst_ref=dst, send_sem=send, recv_sem=recv,
        device_id={"sp": sp}, device_id_type=MESH,
    )


def tp_copy(src, dst, send, recv, tp):
    return pltpu.make_async_remote_copy(
        src_ref=src, dst_ref=dst, send_sem=send, recv_sem=recv,
        device_id={"tp": tp}, device_id_type=MESH,
    )


def gray(k):
    return lax.rem(k + k // 2 - 2 * (k // 3), 4)


def expert_kernel(
    pk, wg_hbm, wu_hbm, wd_hbm,
    xs_out, ps_out, a_out, dg_out, du_out, ret_out,
    wg, wu, wd, own, oth, xs, ps, acts, dgs, dus,
    psend, precv, pown, rsend, ret,
    sel_a, sel_b,
    w_sem, a_send, b_send, c_send, own_sem, oth_sem,
    e_send, e_recv, r_send, r_recv, o_sem,
):
    me = lax.axis_index("sp")
    tp = lax.axis_index("tp")
    peer = 1 - tp
    mx, my, mz = lax.rem(me, 4), lax.rem(me // 4, 4), me // 16
    twin = me + 1 - 2 * lax.rem(me, 2)
    loads = [
        pltpu.make_async_copy(src, dst, w_sem.at[i])
        for i, (src, dst) in enumerate(((wg_hbm, wg), (wu_hbm, wu), (wd_hbm, wd)))
    ]
    for copy in loads:
        copy.start()

    barrier = pltpu.get_barrier_semaphore()

    def greet(k, _):
        pl.semaphore_signal(
            barrier, inc=1, device_id={"sp": lax.rem(me + k, 64)}, device_id_type=MESH
        )
        return 0

    lax.fori_loop(1, 64, greet, 0)
    pl.semaphore_signal(barrier, inc=1, device_id={"tp": peer}, device_id_type=MESH)

    row = lax.broadcasted_iota(jnp.int32, (64, 128), 0)
    col = lax.broadcasted_iota(jnp.int32, (64, 128), 1)
    spot = (row // 4) * 8 + row % 4
    sel_a[...] = (col == spot).astype(F32).astype(BF16)
    sel_b[...] = (col == spot + 4).astype(F32).astype(BF16)
    own[pl.ds(me, 1)] = pk[pl.ds(me // 2, 1)]

    pl.semaphore_wait(barrier, 64)

    def direct_send(i):
        k, j = i // 8, lax.rem(i, 8)
        dz, dy, side = gray(k), gray(j // 2), lax.rem(j, 2)
        x = mx + side * (3 - 2 * mx)
        to = lax.rem(mz + dz, 4) * 16 + lax.rem(my + dy, 4) * 4 + x
        return sp_copy(pk.at[to // 2], own.at[me], a_send.at[i], own_sem.at[me], to)

    def start_direct(i, _):
        direct_send(i).start()
        return 0

    lax.fori_loop(1, 32, start_direct, 0)

    def source(k, j, near):
        dz, dy, side = gray(k), gray(j // 2), lax.rem(j, 2)
        x = mx + side * (3 - 2 * mx)
        twin_x = x + 1 - 2 * lax.rem(x, 2)
        x = x if near else twin_x
        return lax.rem(mz - dz + 4, 4) * 16 + lax.rem(my - dy + 4, 4) * 4 + x

    def twin_copy(i):
        s = source(i // 8, lax.rem(i, 8), True)
        return sp_copy(own.at[s], own.at[s], b_send.at[i], own_sem.at[s], twin)

    def core_copy(s):
        return tp_copy(own.at[s], oth.at[s], c_send.at[s], oth_sem.at[s], peer)

    def arrived(s):
        return sp_copy(own.at[s], own.at[s], c_send.at[s], own_sem.at[s], twin)

    def take_direct(k):
        def one(j, _):
            s = source(k, j, True)

            @pl.when(k * 8 + j != 0)
            def _():
                arrived(s).wait_recv()

            twin_copy(k * 8 + j).start()
            core_copy(s).start()
            return 0

        lax.fori_loop(0, 8, one, 0)

    def take_twin(k):
        def one(j, _):
            s = source(k, j, False)
            arrived(s).wait_recv()
            core_copy(s).start()
            return 0

        lax.fori_loop(0, 8, one, 0)

    def part_copy(z):
        return tp_copy(
            psend.at[pl.ds(z * 16, 16)], precv.at[pl.ds(z * 16, 16)],
            e_send.at[z], e_recv.at[z], peer,
        )

    def ret_copy(s):
        return sp_copy(rsend.at[s], ret.at[me], r_send.at[s], r_recv.at[me], s)

    def ret_arrived(s):
        return sp_copy(rsend.at[s], ret.at[s], r_send.at[s], r_recv.at[s], s)

    def plane(k):
        return lax.rem(mz - gray(k) + 4, 4)

    def compute(k):
        z = plane(k)

        def wait_other(j, _):
            tp_copy(
                own.at[z * 16 + j], oth.at[z * 16 + j],
                c_send.at[z * 16 + j], oth_sem.at[z * 16 + j], peer,
            ).wait_recv()
            return 0

        lax.fori_loop(0, 16, wait_other, 0)
        base = pl.multiple_of(z * 192, 64)
        for buf, half in ((own, tp), (oth, peer)):
            block = buf[pl.ds(z * 16, 16)].reshape(128, 3072)
            left = pl.multiple_of(half * HALF, HALF)
            mid = pl.multiple_of(half * HALF + 512, 512)
            xs[pl.ds(base, 128), pl.ds(left, HALF)] = block[:, :HALF]
            ps[pl.ds(base, 128), pl.ds(left, HALF)] = block[:, HALF : 2 * HALF]
            rest = block[:, 2 * HALF :]
            first = nn(sel_a[...], rest).astype(BF16)
            second = nn(sel_b[...], rest).astype(BF16)
            low = pl.multiple_of(base + 128, 64)
            xs[pl.ds(low, 64), pl.ds(left, 512)] = first[:, :512]
            xs[pl.ds(low, 64), pl.ds(mid, 512)] = second[:, :512]
            ps[pl.ds(low, 64), pl.ds(left, 512)] = first[:, 512:]
            ps[pl.ds(low, 64), pl.ds(mid, 512)] = second[:, 512:]
        x = xs[pl.ds(base, 192), :]
        p = ps[pl.ds(base, 192), :]
        g = nn(x, wg[...])
        u = nn(x, wu[...])
        dh = nt(p, wd[...])
        sig = jax.nn.sigmoid(g)
        silu = g * sig
        acts[pl.ds(base, 192), :] = (silu * u).astype(BF16)
        dg = (dh * u * sig * (1.0 + g * (1.0 - sig))).astype(BF16)
        du = (dh * silu).astype(BF16)
        dgs[pl.ds(base, 192), :] = dg
        dus[pl.ds(base, 192), :] = du
        for out, half in ((psend, peer), (pown, tp)):
            rows = pl.ds(pl.multiple_of(half * HALF, HALF), HALF)
            back = nt(dg, wg[rows, :]) + nt(du, wu[rows, :])
            back = back.astype(BF16)
            out[pl.ds(z * 16, 16), :, :HALF] = back[:128].reshape(16, 8, HALF)
            rest = tn(sel_a[...], back[128:, :512]) + tn(sel_b[...], back[128:, 512:])
            out[pl.ds(z * 16, 16), :, HALF:] = rest.astype(BF16).reshape(16, 8, 512)
            if half is peer:
                part_copy(z).start()

    def give_back(k):
        z = plane(k)
        part_copy(z).wait_recv()
        block = pl.ds(z * 16, 16)
        rsend[block] = (pown[block].astype(F32) + precv[block].astype(F32)).astype(BF16)

        def one(j, _):
            s = z * 16 + lax.rem(lax.rem(me, 16) + j, 16)

            @pl.when(s != me)
            def _():
                ret_copy(s).start()

            return 0

        lax.fori_loop(0, 16, one, 0)

    take_direct(0)
    take_direct(1)
    take_twin(0)
    for copy in loads:
        copy.wait()

    def step(k, _):
        @pl.when(k < 2)
        def _():
            take_direct(k + 2)

        compute(k)

        @pl.when(k < 3)
        def _():
            take_twin(k + 1)

        @pl.when(k > 0)
        def _():
            give_back(k - 1)

        return 0

    lax.fori_loop(0, 4, step, 0)
    outs = [
        pltpu.make_async_copy(src, dst, o_sem.at[i])
        for i, (src, dst) in enumerate(
            ((xs, xs_out), (ps, ps_out), (acts, a_out), (dgs, dg_out), (dus, du_out))
        )
    ]
    for copy in outs:
        copy.start()
    give_back(3)
    ret[pl.ds(me, 1)] = rsend[pl.ds(me, 1)]

    def finish_sends(i, _):
        @pl.when(i > 0)
        def _():
            direct_send(i).wait_send()

        twin_copy(i).wait_send()
        return 0

    lax.fori_loop(0, 32, finish_sends, 0)

    def finish(s, _):
        core_copy(s).wait_send()

        @pl.when(s != me)
        def _():
            ret_copy(s).wait_send()
            ret_arrived(s).wait_recv()

        return 0

    lax.fori_loop(0, 64, finish, 0)
    for z in range(4):
        part_copy(z).wait_send()
    last = pltpu.make_async_copy(ret, ret_out, o_sem.at[5])
    last.start()
    for copy in outs:
        copy.wait()
    last.wait()


def run_experts(pk, wg, wu, wd):
    hidden = wg.shape[1]
    rows = 768
    out = [
        jax.ShapeDtypeStruct((rows, D), BF16),
        jax.ShapeDtypeStruct((rows, D), BF16),
        jax.ShapeDtypeStruct((rows, hidden), BF16),
        jax.ShapeDtypeStruct((rows, hidden), BF16),
        jax.ShapeDtypeStruct((rows, hidden), BF16),
        jax.ShapeDtypeStruct((64, 8, 1536), BF16),
    ]
    dma = pltpu.SemaphoreType.DMA
    return pl.pallas_call(
        expert_kernel,
        out_shape=out,
        in_specs=[pl.BlockSpec(memory_space=pltpu.VMEM)] + [pl.BlockSpec(memory_space=pl.ANY)] * 3,
        out_specs=[pl.BlockSpec(memory_space=pl.ANY)] * 6,
        scratch_shapes=[
            pltpu.VMEM((D, hidden), BF16),
            pltpu.VMEM((D, hidden), BF16),
            pltpu.VMEM((hidden, D), BF16),
            pltpu.VMEM((64, 8, 3072), BF16),
            pltpu.VMEM((64, 8, 3072), BF16),
            pltpu.VMEM((rows, D), BF16),
            pltpu.VMEM((rows, D), BF16),
            pltpu.VMEM((rows, hidden), BF16),
            pltpu.VMEM((rows, hidden), BF16),
            pltpu.VMEM((rows, hidden), BF16),
            pltpu.VMEM((64, 8, 1536), BF16),
            pltpu.VMEM((64, 8, 1536), BF16),
            pltpu.VMEM((64, 8, 1536), BF16),
            pltpu.VMEM((64, 8, 1536), BF16),
            pltpu.VMEM((64, 8, 1536), BF16),
            pltpu.VMEM((64, 128), BF16),
            pltpu.VMEM((64, 128), BF16),
            dma((3,)), dma((32,)), dma((32,)), dma((64,)), dma((64,)), dma((64,)),
            dma((4,)), dma((4,)), dma((64,)), dma((64,)), dma((6,)),
        ],
        compiler_params=pltpu.CompilerParams(
            collective_id=0, has_side_effects=True, vmem_limit_bytes=56 * 1024 * 1024
        ),
        name="experts",
    )(pk, wg, wu, wd)


def slots_of(route_block, experts):
    tok = route_block.shape[0]
    labels = jnp.arange(experts, dtype=jnp.int32)
    onehot = (route_block[:, :, None] == labels[None, None, :]).astype(F32)
    per_token = jnp.sum(onehot, axis=1)
    earlier = (jnp.arange(tok)[:, None] > jnp.arange(tok)[None, :]).astype(F32)
    before = jnp.dot(earlier, per_token)
    return jnp.sum(onehot * before[:, None, :], axis=2).astype(jnp.int32)


def tables(routes, experts):
    slot = slots_of(routes, experts)
    at = jnp.arange(experts * MAIN, dtype=jnp.int32)[None, None, :]
    base = routes * MAIN + slot
    main = (base[:, :, None] == at) & (slot < MAIN)[:, :, None]
    first = (base[:, :, None] - MAIN == at) & (slot >= MAIN)[:, :, None]
    second = (base[:, :, None] - REM == at) & (slot >= MAIN)[:, :, None]
    return main, first, second


def total_of_pieces(array, axis):
    return lax.all_gather(array, axis).sum(0)


def gather_directly(array, axis, dim):
    peers = lax.axis_size(axis)
    blocks = lax.all_to_all(
        jnp.broadcast_to(array[None], (peers, *array.shape)), axis, 0, 0, tiled=True
    )
    shape = list(array.shape)
    shape[dim] *= peers
    return jnp.moveaxis(blocks, 0, dim).reshape(shape)


def summed_on_arrival(array, axis, dim):
    peers = lax.axis_size(axis)
    before, after = array.shape[:dim], array.shape[dim + 1 :]
    blocks = jnp.moveaxis(array.reshape(*before, peers, -1, *after), dim, 0)
    arrived = lax.all_to_all(blocks, axis, split_axis=0, concat_axis=0, tiled=True)
    return arrived.astype(F32).sum(axis=0)


def on_device(
    conv_out, ln_gain, taps, proj_weight, stream_mid, out_grad,
    routes, route_probs, gate_slabs, up_slabs, down_slabs,
):
    tok_rows = conv_out.shape[0]
    experts = lax.axis_size("sp") // 2
    main, first, second = tables(routes, experts)

    def pick(t):
        return (t[:, 0] | t[:, 1]).astype(BF16)

    def weights(t):
        return jnp.sum(t.astype(F32) * route_probs[:, :, None], axis=(0, 1))[:, None]

    s_main, s_first, s_second = pick(main), pick(first), pick(second)
    p_main, p_rest = weights(main), weights(first) + weights(second)
    rest_mid = tn(s_first, stream_mid[:, :512]) + tn(s_second, stream_mid[:, 512:])
    rest_grad = tn(s_first, out_grad[:, :512]) + tn(s_second, out_grad[:, 512:])
    pk = jnp.concatenate(
        [
            tn(s_main, stream_mid).astype(BF16),
            (tn(s_main, out_grad) * p_main).astype(BF16),
            rest_mid.astype(BF16),
            (rest_grad * p_rest).astype(BF16),
        ],
        axis=1,
    ).reshape(experts, MAIN, 3072)

    xs, ps, acts, dg, du, ret = run_experts(pk, gate_slabs[0], up_slabs[0], down_slabs[0])
    grad_down = tn(acts, ps).astype(BF16)
    grad_gate = tn(xs, dg).astype(BF16)
    grad_up = tn(xs, du).astype(BF16)

    pairs = ret.reshape(experts, 2, MAIN, 1536)
    contrib = 0.0
    for h in range(2):
        rows = pairs[:, h].reshape(experts * MAIN, 1536)
        contrib = contrib + nn(s_main, rows[:, :HALF])
        contrib = contrib + jnp.concatenate(
            [nn(s_first, rows[:, HALF:]), nn(s_second, rows[:, HALF:])], axis=1
        )
    grad_stream = (out_grad.astype(F32) + contrib).astype(BF16)

    values = conv_out.astype(F32)
    row_total = total_of_pieces(jnp.sum(values, axis=1), "tp")
    row_squares = total_of_pieces(jnp.sum(values * values, axis=1), "tp")
    row_mean = row_total[:, None] / D
    row_var = row_squares[:, None] / D - row_mean * row_mean
    inv_std = lax.rsqrt(row_var + 1e-06)
    normed = (values - row_mean) * inv_std
    scaled_z = normed * ln_gain[None, :]
    z_sig = jax.nn.sigmoid(scaled_z)
    activated = (scaled_z * z_sig).astype(BF16)
    whole_stream = gather_directly(grad_stream, "tp", 1)
    grad_act = nn(whole_stream, lax.all_gather(proj_weight, "sp", axis=0, tiled=True))
    grad_normed = grad_act * z_sig * (1.0 + scaled_z * (1.0 - z_sig)) * ln_gain[None, :]
    first_sum = total_of_pieces(jnp.sum(grad_normed, axis=1), "tp")
    second_sum = total_of_pieces(jnp.sum(grad_normed * normed, axis=1), "tp")
    grad_conv = (
        inv_std * (grad_normed - first_sum[:, None] / D - normed * second_sum[:, None] / D)
    ).astype(BF16)
    reach = taps.shape[0] - 1
    following = lax.ppermute(grad_conv[:reach], "sp", [(k, k - 1) for k in range(1, 64)])
    extended = jnp.concatenate([grad_conv, following], axis=0).astype(F32)
    tap_values = taps.astype(F32)
    grad_input = jnp.zeros((tok_rows, grad_conv.shape[1]), F32)
    for offset in range(taps.shape[0]):
        grad_input = grad_input + tap_values[offset][None, :] * extended[offset : offset + tok_rows]
    grad_proj = summed_on_arrival(tn(whole_stream, activated).astype(BF16), "sp", 0)
    return (
        grad_input.astype(BF16), grad_proj, grad_gate[None], grad_up[None], grad_down[None],
    )


def solution(mesh):
    return jax.shard_map(
        on_device,
        mesh=mesh,
        in_specs=(
            P("sp", "tp"), P("tp"), P(None, "tp"), P("sp", "tp"), P("sp", "tp"), P("sp", "tp"),
            P("sp", None), P("sp", None), P("sp", None, "tp"), P("sp", None, "tp"), P("sp", "tp", None),
        ),
        out_specs=(
            P("sp", "tp"), P("sp", "tp"), P("sp", None, "tp"), P("sp", None, "tp"), P("sp", "tp", None),
        ),
        check_vma=False,
    )
```

```python
import functools

import jax
import jax.numpy as jnp
from jax import lax
from jax.experimental import pallas as pl
from jax.experimental.pallas import tpu as pltpu
from jax.sharding import PartitionSpec as P

D = 2048
HALF = 1024
MAIN = 8
REM = 4
MESH = pl.DeviceIdType.MESH
F32 = jnp.float32
BF16 = jnp.bfloat16


def nt(a, b):
    return lax.dot_general(a, b, (((1,), (1,)), ((), ())), preferred_element_type=F32)


def nn(a, b):
    return lax.dot_general(a, b, (((1,), (0,)), ((), ())), preferred_element_type=F32)


def tn(a, b):
    return lax.dot_general(a, b, (((0,), (0,)), ((), ())), preferred_element_type=F32)


def sp_copy(src, dst, send, recv, sp):
    return pltpu.make_async_remote_copy(
        src_ref=src, dst_ref=dst, send_sem=send, recv_sem=recv,
        device_id={"sp": sp}, device_id_type=MESH,
    )


def tp_copy(src, dst, send, recv, tp):
    return pltpu.make_async_remote_copy(
        src_ref=src, dst_ref=dst, send_sem=send, recv_sem=recv,
        device_id={"tp": tp}, device_id_type=MESH,
    )


def gray(k):
    return lax.rem(k + k // 2 - 2 * (k // 3), 4)


def expert_kernel(
    pk, conv, gain, wg_hbm, wu_hbm, wd_hbm, proj_hbm,
    xs_out, ps_out, a_out, dg_out, du_out, ret_out, proj_out, act_out, stats_out,
    wg, wu, wd, own, oth, xs, ps, acts, dgs, dus,
    psend, precv, pown, rsend, ret,
    sel_a, sel_b, proj, act, stat_send, stat_recv, stats,
    w_sem, a_send, b_send, c_send, own_sem, oth_sem,
    e_send, e_recv, r_send, r_recv, o_sem,
    g_send, g_recv, s_send, s_recv, t_send, t_recv,
):
    me = lax.axis_index("sp")
    tp = lax.axis_index("tp")
    peer = 1 - tp
    mx, my, mz = lax.rem(me, 4), lax.rem(me // 4, 4), me // 16
    twin = me + 1 - 2 * lax.rem(me, 2)
    loads = [
        pltpu.make_async_copy(src, dst, w_sem.at[i])
        for i, (src, dst) in enumerate(((wg_hbm, wg), (wu_hbm, wu), (wd_hbm, wd)))
    ]
    proj_load = pltpu.make_async_copy(proj_hbm, proj.at[mz, my, mx], w_sem.at[3])
    proj_load.start()
    for copy in loads:
        copy.start()

    barrier = pltpu.get_barrier_semaphore()

    def greet(k, _):
        pl.semaphore_signal(
            barrier, inc=1, device_id={"sp": lax.rem(me + k, 64)}, device_id_type=MESH
        )
        return 0

    lax.fori_loop(1, 64, greet, 0)
    pl.semaphore_signal(barrier, inc=1, device_id={"tp": peer}, device_id_type=MESH)

    row = lax.broadcasted_iota(jnp.int32, (64, 128), 0)
    col = lax.broadcasted_iota(jnp.int32, (64, 128), 1)
    spot = (row // 4) * 8 + row % 4
    sel_a[...] = (col == spot).astype(F32).astype(BF16)
    sel_b[...] = (col == spot + 4).astype(F32).astype(BF16)
    own[pl.ds(me, 1)] = pk[pl.ds(me // 2, 1)]
    values = conv[...].astype(F32)
    lane = lax.broadcasted_iota(jnp.int32, (128, 128), 1)
    total = jnp.sum(values, axis=1, keepdims=True)
    squares = jnp.sum(values * values, axis=1, keepdims=True)
    stat_send[...] = jnp.where(lane == 0, total, squares)
    proj_load.wait()

    pl.semaphore_wait(barrier, 64)

    def direct_send(i):
        k, j = i // 8, lax.rem(i, 8)
        dz, dy, side = gray(k), gray(j // 2), lax.rem(j, 2)
        x = mx + side * (3 - 2 * mx)
        to = lax.rem(mz + dz, 4) * 16 + lax.rem(my + dy, 4) * 4 + x
        return sp_copy(pk.at[to // 2], own.at[me], a_send.at[i], own_sem.at[me], to)

    def start_direct(i, _):
        direct_send(i).start()
        return 0

    lax.fori_loop(1, 32, start_direct, 0)
    stat_copy = tp_copy(stat_send, stat_recv, s_send, s_recv, peer)
    stat_copy.start()

    def gather(group, axis, part):
        def at(d):
            z, y, x = mz, my, mx
            if axis == 0:
                z = lax.rem(mz + d, 4)
            elif axis == 1:
                y = lax.rem(my + d, 4)
            else:
                x = lax.rem(mx + d, 4)
            return z, y, x

        def copy(d, send):
            z, y, x = at(0) if send else at(4 - d)
            to_z, to_y, to_x = at(d)
            block = proj.at[part(z, y, x)]
            return sp_copy(
                block, block, g_send.at[group, d - 1], g_recv.at[group, d - 1],
                to_z * 16 + to_y * 4 + to_x,
            )

        def start():
            for d in (1, 3, 2):
                copy(d, True).start()

        def take():
            for d in (1, 3, 2):
                copy(d, False).wait_recv()

        def sent():
            for d in (1, 3, 2):
                copy(d, True).wait_send()

        return start, take, sent

    every = slice(None)
    low, mid_cols, high = pl.ds(0, 256), pl.ds(256, 512), pl.ds(768, 256)
    first_hop = (
        gather(0, 2, lambda z, y, x: (z, y, x, every, pl.ds(0, 768))),
        gather(1, 1, lambda z, y, x: (z, y, x, every, high)),
    )
    second_hop = (
        gather(2, 1, lambda z, y, x: (z, y, every, every, low)),
        gather(3, 0, lambda z, y, x: (z, y, every, every, mid_cols)),
        gather(4, 0, lambda z, y, x: (z, every, x, every, high)),
    )
    third_hop = (
        gather(5, 0, lambda z, y, x: (z, every, every, every, low)),
        gather(6, 1, lambda z, y, x: (every, y, every, every, mid_cols)),
        gather(7, 2, lambda z, y, x: (every, every, x, every, high)),
    )
    for start, _, _ in first_hop:
        start()

    stat_copy.wait_recv()
    both = stat_send[...] + stat_recv[...]
    row_mean = both[:, 0:1] / D
    row_var = both[:, 1:2] / D - row_mean * row_mean
    inv_std = lax.rsqrt(row_var + 1e-06)
    stats[...] = jnp.where(lane == 0, row_mean, inv_std)
    scaled_z = (values - row_mean) * inv_std * gain[...]
    act[pl.ds(mz, 1)] = (scaled_z * jax.nn.sigmoid(scaled_z)).astype(BF16)[None]

    def act_copy(d, send):
        z = mz if send else lax.rem(mz + 4 - d, 4)
        return sp_copy(
            act.at[z], act.at[z], t_send.at[d - 1], t_recv.at[d - 1],
            lax.rem(mz + d, 4) * 16 + lax.rem(me, 16),
        )

    def source(k, j, near):
        dz, dy, side = gray(k), gray(j // 2), lax.rem(j, 2)
        x = mx + side * (3 - 2 * mx)
        twin_x = x + 1 - 2 * lax.rem(x, 2)
        x = x if near else twin_x
        return lax.rem(mz - dz + 4, 4) * 16 + lax.rem(my - dy + 4, 4) * 4 + x

    def twin_copy(i):
        s = source(i // 8, lax.rem(i, 8), True)
        return sp_copy(own.at[s], own.at[s], b_send.at[i], own_sem.at[s], twin)

    def core_copy(s):
        return tp_copy(own.at[s], oth.at[s], c_send.at[s], oth_sem.at[s], peer)

    def arrived(s):
        return sp_copy(own.at[s], own.at[s], c_send.at[s], own_sem.at[s], twin)

    def take_direct(k):
        def one(j, _):
            s = source(k, j, True)

            @pl.when(k * 8 + j != 0)
            def _():
                arrived(s).wait_recv()

            twin_copy(k * 8 + j).start()
            core_copy(s).start()
            return 0

        lax.fori_loop(0, 8, one, 0)

    def take_twin(k):
        def one(j, _):
            s = source(k, j, False)
            arrived(s).wait_recv()
            core_copy(s).start()
            return 0

        lax.fori_loop(0, 8, one, 0)

    def part_copy(z):
        return tp_copy(
            psend.at[pl.ds(z * 16, 16)], precv.at[pl.ds(z * 16, 16)],
            e_send.at[z], e_recv.at[z], peer,
        )

    def slot(s):
        return lax.rem(s, 2) * 32 + s // 2

    def ret_copy(s):
        return sp_copy(rsend.at[s], ret.at[slot(me)], r_send.at[s], r_recv.at[me], s)

    def ret_arrived(s):
        return sp_copy(rsend.at[s], ret.at[slot(s)], r_send.at[s], r_recv.at[s], s)

    def plane(k):
        return lax.rem(mz - gray(k) + 4, 4)

    def compute(k):
        z = plane(k)

        def wait_other(j, _):
            tp_copy(
                own.at[z * 16 + j], oth.at[z * 16 + j],
                c_send.at[z * 16 + j], oth_sem.at[z * 16 + j], peer,
            ).wait_recv()
            return 0

        lax.fori_loop(0, 16, wait_other, 0)
        base = pl.multiple_of(z * 192, 64)
        for buf, half in ((own, tp), (oth, peer)):
            block = buf[pl.ds(z * 16, 16)].reshape(128, 3072)
            left = pl.multiple_of(half * HALF, HALF)
            mid = pl.multiple_of(half * HALF + 512, 512)
            xs[pl.ds(base, 128), pl.ds(left, HALF)] = block[:, :HALF]
            ps[pl.ds(base, 128), pl.ds(left, HALF)] = block[:, HALF : 2 * HALF]
            rest = block[:, 2 * HALF :]
            first = nn(sel_a[...], rest).astype(BF16)
            second = nn(sel_b[...], rest).astype(BF16)
            low = pl.multiple_of(base + 128, 64)
            xs[pl.ds(low, 64), pl.ds(left, 512)] = first[:, :512]
            xs[pl.ds(low, 64), pl.ds(mid, 512)] = second[:, :512]
            ps[pl.ds(low, 64), pl.ds(left, 512)] = first[:, 512:]
            ps[pl.ds(low, 64), pl.ds(mid, 512)] = second[:, 512:]
        x = xs[pl.ds(base, 192), :]
        p = ps[pl.ds(base, 192), :]
        g = nn(x, wg[...])
        u = nn(x, wu[...])
        dh = nt(p, wd[...])
        sig = jax.nn.sigmoid(g)
        silu = g * sig
        acts[pl.ds(base, 192), :] = (silu * u).astype(BF16)
        dg = (dh * u * sig * (1.0 + g * (1.0 - sig))).astype(BF16)
        du = (dh * silu).astype(BF16)
        dgs[pl.ds(base, 192), :] = dg
        dus[pl.ds(base, 192), :] = du
        for out, half in ((psend, peer), (pown, tp)):
            rows = pl.ds(pl.multiple_of(half * HALF, HALF), HALF)
            back = nt(dg, wg[rows, :]) + nt(du, wu[rows, :])
            back = back.astype(BF16)
            out[pl.ds(z * 16, 16), :, :HALF] = back[:128].reshape(16, 8, HALF)
            rest = tn(sel_a[...], back[128:, :512]) + tn(sel_b[...], back[128:, 512:])
            out[pl.ds(z * 16, 16), :, HALF:] = rest.astype(BF16).reshape(16, 8, 512)
            if half is peer:
                part_copy(z).start()

    def give_back(k):
        z = plane(k)
        part_copy(z).wait_recv()
        block = pl.ds(z * 16, 16)
        rsend[block] = (pown[block].astype(F32) + precv[block].astype(F32)).astype(BF16)

        def one(j, _):
            s = z * 16 + lax.rem(lax.rem(me, 16) + j, 16)

            @pl.when(s != me)
            def _():
                ret_copy(s).start()

            return 0

        lax.fori_loop(0, 16, one, 0)

    take_direct(0)
    take_direct(1)
    for d in (1, 3, 2):
        act_copy(d, True).start()
    for _, take, _ in first_hop:
        take()
    for start, _, _ in second_hop:
        start()
    take_twin(0)
    for copy in loads:
        copy.wait()

    def step(k, _):
        @pl.when(k < 2)
        def _():
            take_direct(k + 2)

        compute(k)

        @pl.when(k < 3)
        def _():
            take_twin(k + 1)

        @pl.when(k > 0)
        def _():
            give_back(k - 1)

        @pl.when(k == 1)
        def _():
            for _, take, _ in second_hop:
                take()
            for start, _, _ in third_hop:
                start()

        return 0

    lax.fori_loop(0, 4, step, 0)
    outs = [
        pltpu.make_async_copy(src, dst, o_sem.at[i])
        for i, (src, dst) in enumerate(
            ((xs, xs_out), (ps, ps_out), (acts, a_out), (dgs, dg_out), (dus, du_out), (stats, stats_out))
        )
    ]
    for copy in outs:
        copy.start()
    give_back(3)
    ret[pl.ds(slot(me), 1)] = rsend[pl.ds(me, 1)]
    for _, take, _ in third_hop:
        take()
    for d in (1, 2, 3):
        act_copy(d, False).wait_recv()
    more = [
        pltpu.make_async_copy(src, dst, o_sem.at[6 + i])
        for i, (src, dst) in enumerate(((proj, proj_out), (act, act_out)))
    ]
    for copy in more:
        copy.start()

    def finish_sends(i, _):
        @pl.when(i > 0)
        def _():
            direct_send(i).wait_send()

        twin_copy(i).wait_send()
        return 0

    lax.fori_loop(0, 32, finish_sends, 0)

    def finish(s, _):
        core_copy(s).wait_send()

        @pl.when(s != me)
        def _():
            ret_copy(s).wait_send()
            ret_arrived(s).wait_recv()

        return 0

    lax.fori_loop(0, 64, finish, 0)
    for z in range(4):
        part_copy(z).wait_send()
    for _, _, sent in first_hop + second_hop + third_hop:
        sent()
    for d in (1, 2, 3):
        act_copy(d, True).wait_send()
    stat_copy.wait_send()
    last = pltpu.make_async_copy(ret, ret_out, o_sem.at[8])
    last.start()
    for copy in more:
        copy.wait()
    for copy in outs:
        copy.wait()
    last.wait()


def run_experts(pk, conv, gain, wg, wu, wd, proj):
    hidden = wg.shape[1]
    rows = 768
    out = [
        jax.ShapeDtypeStruct((rows, D), BF16),
        jax.ShapeDtypeStruct((rows, D), BF16),
        jax.ShapeDtypeStruct((rows, hidden), BF16),
        jax.ShapeDtypeStruct((rows, hidden), BF16),
        jax.ShapeDtypeStruct((rows, hidden), BF16),
        jax.ShapeDtypeStruct((64, 8, 1536), BF16),
        jax.ShapeDtypeStruct((4, 4, 4, 32, HALF), BF16),
        jax.ShapeDtypeStruct((4, 128, HALF), BF16),
        jax.ShapeDtypeStruct((128, 128), F32),
    ]
    dma = pltpu.SemaphoreType.DMA
    return pl.pallas_call(
        expert_kernel,
        out_shape=out,
        in_specs=[pl.BlockSpec(memory_space=pltpu.VMEM)] * 3 + [pl.BlockSpec(memory_space=pl.ANY)] * 4,
        out_specs=[pl.BlockSpec(memory_space=pl.ANY)] * 9,
        scratch_shapes=[
            pltpu.VMEM((D, hidden), BF16),
            pltpu.VMEM((D, hidden), BF16),
            pltpu.VMEM((hidden, D), BF16),
            pltpu.VMEM((64, 8, 3072), BF16),
            pltpu.VMEM((64, 8, 3072), BF16),
            pltpu.VMEM((rows, D), BF16),
            pltpu.VMEM((rows, D), BF16),
            pltpu.VMEM((rows, hidden), BF16),
            pltpu.VMEM((rows, hidden), BF16),
            pltpu.VMEM((rows, hidden), BF16),
            pltpu.VMEM((64, 8, 1536), BF16),
            pltpu.VMEM((64, 8, 1536), BF16),
            pltpu.VMEM((64, 8, 1536), BF16),
            pltpu.VMEM((64, 8, 1536), BF16),
            pltpu.VMEM((64, 8, 1536), BF16),
            pltpu.VMEM((64, 128), BF16),
            pltpu.VMEM((64, 128), BF16),
            pltpu.VMEM((4, 4, 4, 32, HALF), BF16),
            pltpu.VMEM((4, 128, HALF), BF16),
            pltpu.VMEM((128, 128), F32),
            pltpu.VMEM((128, 128), F32),
            pltpu.VMEM((128, 128), F32),
            dma((4,)), dma((32,)), dma((32,)), dma((64,)), dma((64,)), dma((64,)),
            dma((4,)), dma((4,)), dma((64,)), dma((64,)), dma((9,)),
            dma((8, 3)), dma((8, 3)), dma, dma, dma((3,)), dma((3,)),
        ],
        compiler_params=pltpu.CompilerParams(
            collective_id=0, has_side_effects=True, vmem_limit_bytes=56 * 1024 * 1024
        ),
        name="experts",
    )(pk, conv, gain, wg, wu, wd, proj)


def tail_kernel(
    s_main, s_first, s_second, out_grad, conv, gain, taps, stats_in, ret_hbm, proj_hbm, act_hbm,
    gin_out, gproj_out,
    ret, proj, act, gs, gz, part, parts, ext, sum_send, sum_recv, taps_f,
    l_sem, c_send, c_recv, z_send, z_recv, p_send, p_recv, u_send, u_recv, h_send, h_recv,
):
    me = lax.axis_index("sp")
    tp = lax.axis_index("tp")
    peer = 1 - tp
    mz, here = me // 16, lax.rem(me, 16)
    loads = [
        pltpu.make_async_copy(src, dst, l_sem.at[i])
        for i, (src, dst) in enumerate(((ret_hbm, ret), (proj_hbm, proj), (act_hbm, act)))
    ]
    for copy in loads:
        copy.start()
    barrier = pltpu.get_barrier_semaphore()

    def greet(to):
        pl.semaphore_signal(barrier, inc=1, device_id={"sp": to}, device_id_type=MESH)

    def plane_peer(d):
        return lax.rem(mz + d, 4) * 16 + here

    def greet_plane(d, _):
        greet(mz * 16 + lax.rem(here + d, 16))
        return 0

    lax.fori_loop(1, 16, greet_plane, 0)
    for d in (1, 2, 3):
        for core in (0, 1):
            pl.semaphore_signal(
                barrier, inc=1, device_id={"sp": plane_peer(d), "tp": core}, device_id_type=MESH
            )
    greet(lax.rem(me + 1, 64))
    greet(lax.rem(me + 63, 64))
    pl.semaphore_signal(barrier, inc=1, device_id={"tp": peer}, device_id_type=MESH)

    loads[0].wait()
    contrib = jnp.zeros((128, HALF), F32)
    halves = []
    for h in range(2):
        block = ret[pl.ds(h * 32, 32)].reshape(256, 1536)
        contrib = contrib + nn(s_main[...], block[:, :HALF])
        halves.append(block[:, HALF:])
    left = nn(s_first[...], halves[0]) + nn(s_first[...], halves[1])
    right = nn(s_second[...], halves[0]) + nn(s_second[...], halves[1])
    left = (out_grad[:, :512].astype(F32) + (contrib[:, :512] + left)).astype(BF16)
    right = (out_grad[:, 512:].astype(F32) + (contrib[:, 512:] + right)).astype(BF16)
    gs[pl.ds(2 * tp, 1)] = left[None]
    gs[pl.ds(2 * tp + 1, 1)] = right[None]
    pl.semaphore_wait(barrier, 24)

    def core_copy(tp_of):
        rows = pl.ds(2 * tp_of, 2)
        return tp_copy(gs.at[rows], gs.at[rows], c_send, c_recv, peer)

    def plane_copy(z, core, i):
        return pltpu.make_async_remote_copy(
            src_ref=gs.at[z], dst_ref=gz.at[mz],
            send_sem=z_send.at[i, core], recv_sem=z_recv.at[mz],
            device_id={"sp": z * 16 + here, "tp": core}, device_id_type=MESH,
        )

    def plane_arrived(z):
        return sp_copy(gz.at[z], gz.at[z], z_send.at[0, 0], z_recv.at[z], z * 16 + here)

    core_copy(tp).start()
    for i in range(2):
        z = 2 * tp + i

        @pl.when(z != mz)
        def _():
            plane_copy(z, 0, i).start()
            plane_copy(z, 1, i).start()

    loads[1].wait()
    loads[2].wait()

    def weights(z):
        return proj[pl.ds(z, 1)].reshape(512, HALF)

    grad_act = nn(left, weights(2 * tp)) + nn(right, weights(2 * tp + 1))
    core_copy(peer).wait_recv()
    mine = gs[pl.ds(mz, 1)].reshape(128, 512)
    total = tn(mine, act[pl.ds(mz, 1)].reshape(128, HALF))
    for d in (1, 3, 2):
        z = lax.rem(mz + d, 4)
        plane_arrived(z).wait_recv()
        total = total + tn(gz[pl.ds(z, 1)].reshape(128, 512), act[pl.ds(z, 1)].reshape(128, HALF))
    part[...] = total.astype(BF16).reshape(16, 32, HALF)

    def part_copy(d):
        q = lax.rem(here + d, 16)
        return sp_copy(part.at[q], parts.at[here], p_send.at[d], p_recv.at[here], mz * 16 + q)

    def part_arrived(q):
        return sp_copy(parts.at[q], parts.at[q], p_send.at[0], p_recv.at[q], mz * 16 + q)

    def start_part(d, _):
        part_copy(d).start()
        return 0

    other = gs[pl.ds(2 * peer, 2)]
    grad_act = grad_act + nn(other[0], weights(2 * peer)) + nn(other[1], weights(2 * peer + 1))
    lax.fori_loop(1, 16, start_part, 0)

    row_mean, inv_std = stats_in[:, 0:1], stats_in[:, 1:2]
    normed = (conv[...].astype(F32) - row_mean) * inv_std
    scaled_z = normed * gain[...]
    z_sig = jax.nn.sigmoid(scaled_z)
    grad_normed = grad_act * z_sig * (1.0 + scaled_z * (1.0 - z_sig)) * gain[...]
    lane = lax.broadcasted_iota(jnp.int32, (128, 128), 1)
    sum_send[...] = jnp.where(
        lane == 0,
        jnp.sum(grad_normed, axis=1, keepdims=True),
        jnp.sum(grad_normed * normed, axis=1, keepdims=True),
    )
    taps_f[pl.ds(0, 31), :] = taps[...].astype(F32)
    sum_copy = tp_copy(sum_send, sum_recv, u_send, u_recv, peer)
    sum_copy.start()
    sum_copy.wait_recv()
    both = sum_send[...] + sum_recv[...]
    grad_conv = inv_std * (grad_normed - both[:, 0:1] / D - normed * (both[:, 1:2] / D))
    ext[pl.ds(0, 128), :] = grad_conv.astype(BF16).astype(F32)

    def reach_copy(to):
        return sp_copy(ext.at[pl.ds(0, 32)], ext.at[pl.ds(128, 32)], h_send, h_recv, to)

    @pl.when(me == 63)
    def _():
        ext[pl.ds(128, 32), :] = jnp.zeros((32, HALF), F32)

    @pl.when(me > 0)
    def _():
        reach_copy(me - 1).start()

    parts[pl.ds(here, 1)] = part[pl.ds(here, 1)]

    @pl.when(me < 63)
    def _():
        reach_copy(me + 1).wait_recv()

    def columns(c, _):
        cols = pl.ds(pl.multiple_of(c * 128, 128), 128)
        acc = jnp.zeros((128, 128), F32)
        for k in range(31):
            acc = acc + taps_f[pl.ds(k, 1), cols] * ext[pl.ds(k, 128), cols]
        gin_out[:, cols] = acc.astype(BF16)
        return 0

    lax.fori_loop(0, 8, columns, 0)

    def wait_part(d, _):
        part_arrived(lax.rem(here + d, 16)).wait_recv()
        return 0

    lax.fori_loop(1, 16, wait_part, 0)
    result = parts[0].astype(F32)
    for q in range(1, 16):
        result = result + parts[q].astype(F32)
    gproj_out[...] = result

    def sent_part(d, _):
        part_copy(d).wait_send()
        return 0

    lax.fori_loop(1, 16, sent_part, 0)
    core_copy(tp).wait_send()
    sum_copy.wait_send()
    for i in range(2):
        z = 2 * tp + i

        @pl.when(z != mz)
        def _():
            plane_copy(z, 0, i).wait_send()
            plane_copy(z, 1, i).wait_send()

    @pl.when(me > 0)
    def _():
        reach_copy(me - 1).wait_send()


def run_tail(s_main, s_first, s_second, out_grad, conv, gain, taps, stats, ret, proj, act):
    dma = pltpu.SemaphoreType.DMA
    return pl.pallas_call(
        tail_kernel,
        out_shape=[
            jax.ShapeDtypeStruct((128, HALF), BF16),
            jax.ShapeDtypeStruct((32, HALF), F32),
        ],
        in_specs=[pl.BlockSpec(memory_space=pltpu.VMEM)] * 8 + [pl.BlockSpec(memory_space=pl.ANY)] * 3,
        out_specs=[pl.BlockSpec(memory_space=pltpu.VMEM)] * 2,
        scratch_shapes=[
            pltpu.VMEM((64, 8, 1536), BF16),
            pltpu.VMEM((4, 4, 4, 32, HALF), BF16),
            pltpu.VMEM((4, 128, HALF), BF16),
            pltpu.VMEM((4, 128, 512), BF16),
            pltpu.VMEM((4, 128, 512), BF16),
            pltpu.VMEM((16, 32, HALF), BF16),
            pltpu.VMEM((16, 32, HALF), BF16),
            pltpu.VMEM((160, HALF), F32),
            pltpu.VMEM((128, 128), F32),
            pltpu.VMEM((128, 128), F32),
            pltpu.VMEM((32, HALF), F32),
            dma((3,)), dma, dma, dma((2, 2)), dma((4,)), dma((16,)), dma((16,)),
            dma, dma, dma, dma,
        ],
        compiler_params=pltpu.CompilerParams(
            collective_id=1, has_side_effects=True, vmem_limit_bytes=40 * 1024 * 1024
        ),
        name="tail",
    )(s_main, s_first, s_second, out_grad, conv, gain, taps, stats, ret, proj, act)


def slots_of(route_block, experts):
    tok = route_block.shape[0]
    labels = jnp.arange(experts, dtype=jnp.int32)
    onehot = (route_block[:, :, None] == labels[None, None, :]).astype(F32)
    per_token = jnp.sum(onehot, axis=1)
    earlier = (jnp.arange(tok)[:, None] > jnp.arange(tok)[None, :]).astype(F32)
    before = jnp.dot(earlier, per_token)
    return jnp.sum(onehot * before[:, None, :], axis=2).astype(jnp.int32)


def tables(routes, experts):
    slot = slots_of(routes, experts)
    at = jnp.arange(experts * MAIN, dtype=jnp.int32)[None, None, :]
    base = routes * MAIN + slot
    main = (base[:, :, None] == at) & (slot < MAIN)[:, :, None]
    first = (base[:, :, None] - MAIN == at) & (slot >= MAIN)[:, :, None]
    second = (base[:, :, None] - REM == at) & (slot >= MAIN)[:, :, None]
    return main, first, second


def on_device(
    conv_out, ln_gain, taps, proj_weight, stream_mid, out_grad,
    routes, route_probs, gate_slabs, up_slabs, down_slabs,
):
    experts = lax.axis_size("sp") // 2
    main, first, second = tables(routes, experts)

    def pick(t):
        return (t[:, 0] | t[:, 1]).astype(BF16)

    def weights(t):
        return jnp.sum(t.astype(F32) * route_probs[:, :, None], axis=(0, 1))[:, None]

    s_main, s_first, s_second = pick(main), pick(first), pick(second)
    p_main, p_rest = weights(main), weights(first) + weights(second)
    rest_mid = tn(s_first, stream_mid[:, :512]) + tn(s_second, stream_mid[:, 512:])
    rest_grad = tn(s_first, out_grad[:, :512]) + tn(s_second, out_grad[:, 512:])
    pk = jnp.concatenate(
        [
            tn(s_main, stream_mid).astype(BF16),
            (tn(s_main, out_grad) * p_main).astype(BF16),
            rest_mid.astype(BF16),
            (rest_grad * p_rest).astype(BF16),
        ],
        axis=1,
    ).reshape(experts, MAIN, 3072)

    gain = ln_gain[None, :]
    xs, ps, acts, dg, du, ret, proj, act, stats = run_experts(
        pk, conv_out, gain, gate_slabs[0], up_slabs[0], down_slabs[0], proj_weight
    )
    grad_input, grad_proj = run_tail(
        s_main, s_first, s_second, out_grad, conv_out, gain, taps, stats, ret, proj, act
    )
    grad_down = tn(acts, ps).astype(BF16)
    grad_gate = tn(xs, dg).astype(BF16)
    grad_up = tn(xs, du).astype(BF16)
    return (
        grad_input, grad_proj, grad_gate[None], grad_up[None], grad_down[None],
    )


def solution(mesh):
    return jax.shard_map(
        on_device,
        mesh=mesh,
        in_specs=(
            P("sp", "tp"), P("tp"), P(None, "tp"), P("sp", "tp"), P("sp", "tp"), P("sp", "tp"),
            P("sp", None), P("sp", None), P("sp", None, "tp"), P("sp", None, "tp"), P("sp", "tp", None),
        ),
        out_specs=(
            P("sp", "tp"), P("sp", "tp"), P("sp", None, "tp"), P("sp", None, "tp"), P("sp", "tp", None),
        ),
        check_vma=False,
    )
```

```python
import functools

import jax
import jax.numpy as jnp
from jax import lax
from jax.experimental import pallas as pl
from jax.experimental.pallas import tpu as pltpu
from jax.sharding import PartitionSpec as P

D = 2048
HALF = 1024
MAIN = 8
REM = 4
MESH = pl.DeviceIdType.MESH
F32 = jnp.float32
BF16 = jnp.bfloat16
VMEM_BYTES = 42 * 1024 * 1024


def nt(a, b):
    return lax.dot_general(a, b, (((1,), (1,)), ((), ())), preferred_element_type=F32)


def nn(a, b):
    return lax.dot_general(a, b, (((1,), (0,)), ((), ())), preferred_element_type=F32)


def tn(a, b):
    return lax.dot_general(a, b, (((0,), (0,)), ((), ())), preferred_element_type=F32)


def sp_copy(src, dst, send, recv, sp):
    return pltpu.make_async_remote_copy(
        src_ref=src, dst_ref=dst, send_sem=send, recv_sem=recv,
        device_id={"sp": sp}, device_id_type=MESH,
    )


def tp_copy(src, dst, send, recv, tp):
    return pltpu.make_async_remote_copy(
        src_ref=src, dst_ref=dst, send_sem=send, recv_sem=recv,
        device_id={"tp": tp}, device_id_type=MESH,
    )


def gray(k):
    return lax.rem(k + k // 2 - 2 * (k // 3), 4)


def layer_kernel(
    routes, probs, stream, out_grad, conv, gain, taps, wg_hbm, wu_hbm, wd_hbm, proj_hbm,
    gin_out, gproj_out, wg, wu, wd,
    pk, own, oth, xs, ps, acts, dgs, dus, psend, precv, pown, ret,
    table, sel_a, sel_b, proj, act, stat_send, stat_recv, stats,
    gs, gz, part, parts, ext, sum_send, sum_recv, taps_f,
    w_sem, a_send, b_send, c_send, own_sem, oth_sem,
    e_send, e_recv, r_send, r_recv,
    g_send, g_recv, s_send, s_recv, t_send, t_recv,
    q_send, q_recv, z_send, z_recv, p_send, p_recv, u_send, u_recv, h_send, h_recv,
):
    me = lax.axis_index("sp")
    tp = lax.axis_index("tp")
    peer = 1 - tp
    mx, my, mz = lax.rem(me, 4), lax.rem(me // 4, 4), me // 16
    here = lax.rem(me, 16)
    twin = me + 1 - 2 * lax.rem(me, 2)
    loads = [
        pltpu.make_async_copy(src, dst, w_sem.at[i])
        for i, (src, dst) in enumerate(((wg_hbm, wg), (wu_hbm, wu), (wd_hbm, wd)))
    ]
    proj_load = pltpu.make_async_copy(proj_hbm, proj.at[mz, my, mx], w_sem.at[3])
    proj_load.start()
    for copy in loads:
        copy.start()

    barrier = pltpu.get_barrier_semaphore()

    def greet(k, _):
        pl.semaphore_signal(
            barrier, inc=1, device_id={"sp": lax.rem(me + k, 64)}, device_id_type=MESH
        )
        return 0

    lax.fori_loop(1, 64, greet, 0)
    pl.semaphore_signal(barrier, inc=1, device_id={"tp": peer}, device_id_type=MESH)
    for d in (1, 2, 3):
        pl.semaphore_signal(
            barrier, inc=1, device_id={"sp": lax.rem(mz + d, 4) * 16 + here, "tp": peer},
            device_id_type=MESH,
        )

    expert = lax.broadcasted_iota(jnp.int32, (128, 128), 0)
    other = lax.broadcasted_iota(jnp.int32, (128, 128), 1)
    picks = [expert == routes[j : j + 1, :] for j in range(2)]
    counts = picks[0].astype(F32) + picks[1].astype(F32)
    before = nn(counts.astype(BF16), (expert < other).astype(F32).astype(BF16))
    at = lax.broadcasted_iota(jnp.int32, (256, 128), 0)
    for j in range(2):
        slot_row = jnp.sum(jnp.where(picks[j], before, 0.0), axis=0, keepdims=True)
        slot_row = slot_row.astype(jnp.int32)
        base = routes[j : j + 1, :] * MAIN + slot_row
        near = jnp.where(slot_row < MAIN, base, -1)
        far = jnp.where(slot_row < MAIN, -1, base)
        table[3 * j] = (at == near).astype(F32).astype(BF16)
        table[3 * j + 1] = (at + MAIN == far).astype(F32).astype(BF16)
        table[3 * j + 2] = (at + REM == far).astype(F32).astype(BF16)
    for i in range(3):
        table[6 + i] = table[i] + table[3 + i]
    shape = (32, 8, HALF)
    pk[:, :, :HALF] = nn(table[6], stream[...]).astype(BF16).reshape(shape)
    rest = nn(table[7], stream[:, :512]) + nn(table[8], stream[:, 512:])
    pk[:, :, 2 * HALF : 2 * HALF + 512] = rest.astype(BF16).reshape(32, 8, 512)
    grads = []
    for j in range(2):
        prob = jnp.broadcast_to(probs[j : j + 1, :], (128, 128)).T[:, 0:1]
        grads.append((out_grad[...].astype(F32) * prob).astype(BF16))
    near = nn(table[0], grads[0]) + nn(table[3], grads[1])
    pk[:, :, HALF : 2 * HALF] = near.astype(BF16).reshape(shape)
    rest = nn(table[1], grads[0][:, :512]) + nn(table[4], grads[1][:, :512])
    rest = rest + nn(table[2], grads[0][:, 512:]) + nn(table[5], grads[1][:, 512:])
    pk[:, :, 2 * HALF + 512 :] = rest.astype(BF16).reshape(32, 8, 512)

    row = lax.broadcasted_iota(jnp.int32, (64, 128), 0)
    col = lax.broadcasted_iota(jnp.int32, (64, 128), 1)
    spot = (row // 4) * 8 + row % 4
    sel_a[...] = (col == spot).astype(F32).astype(BF16)
    sel_b[...] = (col == spot + 4).astype(F32).astype(BF16)
    own[pl.ds(me, 1)] = pk[pl.ds(me // 2, 1)]
    values = conv[...].astype(F32)
    lane = lax.broadcasted_iota(jnp.int32, (128, 128), 1)
    total = jnp.sum(values, axis=1, keepdims=True)
    squares = jnp.sum(values * values, axis=1, keepdims=True)
    stat_send[...] = jnp.where(lane == 0, total, squares)
    proj_load.wait()

    pl.semaphore_wait(barrier, 67)

    def direct_send(i):
        k, j = i // 8, lax.rem(i, 8)
        dz, dy, side = gray(k), gray(j // 2), lax.rem(j, 2)
        x = mx + side * (3 - 2 * mx)
        to = lax.rem(mz + dz, 4) * 16 + lax.rem(my + dy, 4) * 4 + x
        return sp_copy(pk.at[to // 2], own.at[me], a_send.at[i], own_sem.at[me], to)

    def start_direct(i, _):
        direct_send(i).start()
        return 0

    lax.fori_loop(1, 32, start_direct, 0)
    stat_copy = tp_copy(stat_send, stat_recv, s_send, s_recv, peer)
    stat_copy.start()

    def gather(group, axis, part):
        def at(d):
            z, y, x = mz, my, mx
            if axis == 0:
                z = lax.rem(mz + d, 4)
            elif axis == 1:
                y = lax.rem(my + d, 4)
            else:
                x = lax.rem(mx + d, 4)
            return z, y, x

        def copy(d, send):
            z, y, x = at(0) if send else at(4 - d)
            to_z, to_y, to_x = at(d)
            block = proj.at[part(z, y, x)]
            return sp_copy(
                block, block, g_send.at[group, d - 1], g_recv.at[group, d - 1],
                to_z * 16 + to_y * 4 + to_x,
            )

        def start():
            for d in (1, 3, 2):
                copy(d, True).start()

        def take():
            for d in (1, 3, 2):
                copy(d, False).wait_recv()

        def sent():
            for d in (1, 3, 2):
                copy(d, True).wait_send()

        return start, take, sent

    every = slice(None)
    low, mid_cols, high = pl.ds(0, 256), pl.ds(256, 512), pl.ds(768, 256)
    first_hop = (
        gather(0, 2, lambda z, y, x: (z, y, x, every, pl.ds(0, 768))),
        gather(1, 1, lambda z, y, x: (z, y, x, every, high)),
    )
    second_hop = (
        gather(2, 1, lambda z, y, x: (z, y, every, every, low)),
        gather(3, 0, lambda z, y, x: (z, y, every, every, mid_cols)),
        gather(4, 0, lambda z, y, x: (z, every, x, every, high)),
    )
    third_hop = (
        gather(5, 0, lambda z, y, x: (z, every, every, every, low)),
        gather(6, 1, lambda z, y, x: (every, y, every, every, mid_cols)),
        gather(7, 2, lambda z, y, x: (every, every, x, every, high)),
    )
    for start, _, _ in first_hop:
        start()

    stat_copy.wait_recv()
    both = stat_send[...] + stat_recv[...]
    row_mean = both[:, 0:1] / D
    row_var = both[:, 1:2] / D - row_mean * row_mean
    inv_std = lax.rsqrt(row_var + 1e-06)
    stats[...] = jnp.where(lane == 0, row_mean, inv_std)
    scaled_z = (values - row_mean) * inv_std * gain[...]
    act[pl.ds(mz, 1)] = (scaled_z * jax.nn.sigmoid(scaled_z)).astype(BF16)[None]

    def act_copy(d, send):
        z = mz if send else lax.rem(mz + 4 - d, 4)
        return sp_copy(
            act.at[z], act.at[z], t_send.at[d - 1], t_recv.at[d - 1],
            lax.rem(mz + d, 4) * 16 + lax.rem(me, 16),
        )

    def source(k, j, near):
        dz, dy, side = gray(k), gray(j // 2), lax.rem(j, 2)
        x = mx + side * (3 - 2 * mx)
        twin_x = x + 1 - 2 * lax.rem(x, 2)
        x = x if near else twin_x
        return lax.rem(mz - dz + 4, 4) * 16 + lax.rem(my - dy + 4, 4) * 4 + x

    def twin_copy(i):
        s = source(i // 8, lax.rem(i, 8), True)
        return sp_copy(own.at[s], own.at[s], b_send.at[i], own_sem.at[s], twin)

    def core_copy(s):
        return tp_copy(own.at[s], oth.at[s], c_send.at[s], oth_sem.at[s], peer)

    def arrived(s):
        return sp_copy(own.at[s], own.at[s], c_send.at[s], own_sem.at[s], twin)

    def take_direct(k):
        def one(j, _):
            s = source(k, j, True)

            @pl.when(k * 8 + j != 0)
            def _():
                arrived(s).wait_recv()

            twin_copy(k * 8 + j).start()
            core_copy(s).start()
            return 0

        lax.fori_loop(0, 8, one, 0)

    def take_twin(k):
        def one(j, _):
            s = source(k, j, False)
            arrived(s).wait_recv()
            core_copy(s).start()
            return 0

        lax.fori_loop(0, 8, one, 0)

    def part_copy(z):
        return tp_copy(
            psend.at[pl.ds(z * 16, 16)], precv.at[pl.ds(z * 16, 16)],
            e_send.at[z], e_recv.at[z], peer,
        )

    def slot(s):
        return lax.rem(s, 2) * 32 + s // 2

    def ret_copy(s):
        return sp_copy(pown.at[s], ret.at[slot(me)], r_send.at[s], r_recv.at[me], s)

    def ret_arrived(s):
        return sp_copy(pown.at[s], ret.at[slot(s)], r_send.at[s], r_recv.at[s], s)

    def plane(k):
        return lax.rem(mz - gray(k) + 4, 4)

    def compute(k):
        z = plane(k)

        def wait_other(j, _):
            tp_copy(
                own.at[z * 16 + j], oth.at[z * 16 + j],
                c_send.at[z * 16 + j], oth_sem.at[z * 16 + j], peer,
            ).wait_recv()
            return 0

        lax.fori_loop(0, 16, wait_other, 0)
        base = pl.multiple_of(z * 192, 64)
        for buf, half in ((own, tp), (oth, peer)):
            block = buf[pl.ds(z * 16, 16)].reshape(128, 3072)
            left = pl.multiple_of(half * HALF, HALF)
            mid = pl.multiple_of(half * HALF + 512, 512)
            xs[pl.ds(base, 128), pl.ds(left, HALF)] = block[:, :HALF]
            ps[pl.ds(base, 128), pl.ds(left, HALF)] = block[:, HALF : 2 * HALF]
            rest = block[:, 2 * HALF :]
            first = nn(sel_a[...], rest).astype(BF16)
            second = nn(sel_b[...], rest).astype(BF16)
            low = pl.multiple_of(base + 128, 64)
            xs[pl.ds(low, 64), pl.ds(left, 512)] = first[:, :512]
            xs[pl.ds(low, 64), pl.ds(mid, 512)] = second[:, :512]
            ps[pl.ds(low, 64), pl.ds(left, 512)] = first[:, 512:]
            ps[pl.ds(low, 64), pl.ds(mid, 512)] = second[:, 512:]
        x = xs[pl.ds(base, 192), :]
        p = ps[pl.ds(base, 192), :]
        g = nn(x, wg[...])
        u = nn(x, wu[...])
        dh = nt(p, wd[...])
        sig = jax.nn.sigmoid(g)
        silu = g * sig
        acts[pl.ds(base, 192), :] = (silu * u).astype(BF16)
        dg = (dh * u * sig * (1.0 + g * (1.0 - sig))).astype(BF16)
        du = (dh * silu).astype(BF16)
        dgs[pl.ds(base, 192), :] = dg
        dus[pl.ds(base, 192), :] = du
        for out, half in ((psend, peer), (pown, tp)):
            rows = pl.ds(pl.multiple_of(half * HALF, HALF), HALF)
            back = nt(dg, wg[rows, :]) + nt(du, wu[rows, :])
            back = back.astype(BF16)
            out[pl.ds(z * 16, 16), :, :HALF] = back[:128].reshape(16, 8, HALF)
            rest = tn(sel_a[...], back[128:, :512]) + tn(sel_b[...], back[128:, 512:])
            out[pl.ds(z * 16, 16), :, HALF:] = rest.astype(BF16).reshape(16, 8, 512)
            if half is peer:
                part_copy(z).start()

    def give_back(k):
        z = plane(k)
        part_copy(z).wait_recv()
        block = pl.ds(z * 16, 16)
        pown[block] = (pown[block].astype(F32) + precv[block].astype(F32)).astype(BF16)

        def one(j, _):
            s = z * 16 + lax.rem(lax.rem(me, 16) + j, 16)

            @pl.when(s != me)
            def _():
                ret_copy(s).start()

            return 0

        lax.fori_loop(0, 16, one, 0)

    take_direct(0)
    take_direct(1)
    for d in (1, 3, 2):
        act_copy(d, True).start()
    for _, take, _ in first_hop:
        take()
    for start, _, _ in second_hop:
        start()
    take_twin(0)
    for copy in loads:
        copy.wait()

    def step(k, _):
        @pl.when(k < 2)
        def _():
            take_direct(k + 2)

        compute(k)

        @pl.when(k < 3)
        def _():
            take_twin(k + 1)

        @pl.when(k > 0)
        def _():
            give_back(k - 1)

        @pl.when(k == 0)
        def _():
            for _, take, _ in second_hop:
                take()
            for start, _, _ in third_hop[:2]:
                start()

        return 0

    lax.fori_loop(0, 4, step, 0)
    give_back(3)
    ret[pl.ds(slot(me), 1)] = pown[pl.ds(me, 1)]
    third_hop[2][0]()

    def weight_grads(i, _):
        cols = pl.ds(pl.multiple_of(i * 256, 256), 256)
        rows = xs[:, cols].T
        wg[cols, :] = nn(rows, dgs[...]).astype(BF16)
        wu[cols, :] = nn(rows, dus[...]).astype(BF16)
        return 0

    lax.fori_loop(0, 8, weight_grads, 0)

    def down_grads(i, _):
        cols = pl.ds(pl.multiple_of(i * 128, 128), 128)
        wd[cols, :] = nn(acts[:, cols].T, ps[...]).astype(BF16)
        return 0

    lax.fori_loop(0, 7, down_grads, 0)
    taps_f[pl.ds(0, 31), :] = taps[...].astype(F32)

    def await_return(s, _):
        @pl.when(s != me)
        def _():
            ret_arrived(s).wait_recv()

        return 0

    lax.fori_loop(0, 64, await_return, 0)
    contrib = jnp.zeros((128, HALF), F32)
    halves = []
    for h in range(2):
        block = ret[pl.ds(h * 32, 32)].reshape(256, 1536)
        contrib = contrib + tn(table[6], block[:, :HALF])
        halves.append(block[:, HALF:])
    left = tn(table[7], halves[0]) + tn(table[7], halves[1])
    right = tn(table[8], halves[0]) + tn(table[8], halves[1])
    left = (out_grad[:, :512].astype(F32) + (contrib[:, :512] + left)).astype(BF16)
    right = (out_grad[:, 512:].astype(F32) + (contrib[:, 512:] + right)).astype(BF16)
    gs[pl.ds(2 * tp, 1)] = left[None]
    gs[pl.ds(2 * tp + 1, 1)] = right[None]

    def stream_copy(tp_of):
        rows = pl.ds(2 * tp_of, 2)
        return tp_copy(gs.at[rows], gs.at[rows], q_send, q_recv, peer)

    def plane_copy(z, core, i):
        return pltpu.make_async_remote_copy(
            src_ref=gs.at[z], dst_ref=gz.at[mz],
            send_sem=z_send.at[i, core], recv_sem=z_recv.at[mz],
            device_id={"sp": z * 16 + here, "tp": core}, device_id_type=MESH,
        )

    def plane_arrived(z):
        return sp_copy(gz.at[z], gz.at[z], z_send.at[0, 0], z_recv.at[z], z * 16 + here)

    stream_copy(tp).start()
    for i in range(2):
        z = 2 * tp + i

        @pl.when(z != mz)
        def _():
            plane_copy(z, 0, i).start()
            plane_copy(z, 1, i).start()

    for d in (1, 2, 3):
        act_copy(d, False).wait_recv()

    def weights(z):
        return proj[pl.ds(z, 1)].reshape(512, HALF)

    for _, take, _ in third_hop:
        take()
    grad_act = nn(left, weights(2 * tp)) + nn(right, weights(2 * tp + 1))
    stream_copy(peer).wait_recv()
    mine = gs[pl.ds(mz, 1)].reshape(128, 512)
    total = tn(mine, act[pl.ds(mz, 1)].reshape(128, HALF))
    for d in (1, 3, 2):
        z = lax.rem(mz + d, 4)
        plane_arrived(z).wait_recv()
        total = total + tn(gz[pl.ds(z, 1)].reshape(128, 512), act[pl.ds(z, 1)].reshape(128, HALF))
    part[...] = total.astype(BF16).reshape(16, 32, HALF)

    def proj_copy(d):
        q = lax.rem(here + d, 16)
        return sp_copy(part.at[q], parts.at[here], p_send.at[d], p_recv.at[here], mz * 16 + q)

    def part_arrived(q):
        return sp_copy(parts.at[q], parts.at[q], p_send.at[0], p_recv.at[q], mz * 16 + q)

    def start_part(d, _):
        proj_copy(d).start()
        return 0

    other = gs[pl.ds(2 * peer, 2)]
    grad_act = grad_act + nn(other[0], weights(2 * peer)) + nn(other[1], weights(2 * peer + 1))
    lax.fori_loop(1, 16, start_part, 0)

    row_mean, inv_std = stats[:, 0:1], stats[:, 1:2]
    normed = (conv[...].astype(F32) - row_mean) * inv_std
    scaled_z = normed * gain[...]
    z_sig = jax.nn.sigmoid(scaled_z)
    grad_normed = grad_act * z_sig * (1.0 + scaled_z * (1.0 - z_sig)) * gain[...]
    sum_send[...] = jnp.where(
        lane == 0,
        jnp.sum(grad_normed, axis=1, keepdims=True),
        jnp.sum(grad_normed * normed, axis=1, keepdims=True),
    )
    sum_copy = tp_copy(sum_send, sum_recv, u_send, u_recv, peer)
    sum_copy.start()
    sum_copy.wait_recv()
    both = sum_send[...] + sum_recv[...]
    grad_conv = inv_std * (grad_normed - both[:, 0:1] / D - normed * (both[:, 1:2] / D))
    ext[pl.ds(0, 128), :] = grad_conv.astype(BF16).astype(F32)

    def reach_copy(to):
        return sp_copy(ext.at[pl.ds(0, 32)], ext.at[pl.ds(128, 32)], h_send, h_recv, to)

    @pl.when(me == 63)
    def _():
        ext[pl.ds(128, 32), :] = jnp.zeros((32, HALF), F32)

    @pl.when(me > 0)
    def _():
        reach_copy(me - 1).start()

    parts[pl.ds(here, 1)] = part[pl.ds(here, 1)]

    @pl.when(me < 63)
    def _():
        reach_copy(me + 1).wait_recv()

    def columns(c, _):
        cols = pl.ds(pl.multiple_of(c * 128, 128), 128)
        acc = jnp.zeros((128, 128), F32)
        for k in range(31):
            acc = acc + taps_f[pl.ds(k, 1), cols] * ext[pl.ds(k, 128), cols]
        gin_out[:, cols] = acc.astype(BF16)
        return 0

    lax.fori_loop(0, 8, columns, 0)

    def wait_part(d, _):
        part_arrived(lax.rem(here + d, 16)).wait_recv()
        return 0

    lax.fori_loop(1, 16, wait_part, 0)
    result = parts[0].astype(F32)
    for q in range(1, 16):
        result = result + parts[q].astype(F32)
    gproj_out[...] = result

    def sent_part(d, _):
        proj_copy(d).wait_send()
        return 0

    lax.fori_loop(1, 16, sent_part, 0)
    stream_copy(tp).wait_send()
    sum_copy.wait_send()
    for i in range(2):
        z = 2 * tp + i

        @pl.when(z != mz)
        def _():
            plane_copy(z, 0, i).wait_send()
            plane_copy(z, 1, i).wait_send()

    @pl.when(me > 0)
    def _():
        reach_copy(me - 1).wait_send()

    def finish_sends(i, _):
        @pl.when(i > 0)
        def _():
            direct_send(i).wait_send()

        twin_copy(i).wait_send()
        return 0

    lax.fori_loop(0, 32, finish_sends, 0)

    def finish(s, _):
        core_copy(s).wait_send()

        @pl.when(s != me)
        def _():
            ret_copy(s).wait_send()

        return 0

    lax.fori_loop(0, 64, finish, 0)
    for z in range(4):
        part_copy(z).wait_send()
    for _, _, sent in first_hop + second_hop + third_hop:
        sent()
    for d in (1, 2, 3):
        act_copy(d, True).wait_send()
    stat_copy.wait_send()
def on_device(
    conv_out, ln_gain, taps, proj_weight, stream_mid, out_grad,
    routes, route_probs, gate_slabs, up_slabs, down_slabs,
):
    hidden = gate_slabs.shape[2]
    rows = 768
    dma = pltpu.SemaphoreType.DMA
    vmem = pltpu.VMEM
    slots = vmem((64, 8, 1536), BF16)
    grad_input, grad_proj, grad_gate, grad_up, grad_down = pl.pallas_call(
        layer_kernel,
        out_shape=[
            jax.ShapeDtypeStruct((128, HALF), BF16),
            jax.ShapeDtypeStruct((32, HALF), F32),
            jax.ShapeDtypeStruct((D, hidden), BF16),
            jax.ShapeDtypeStruct((D, hidden), BF16),
            jax.ShapeDtypeStruct((hidden, D), BF16),
        ],
        in_specs=[pl.BlockSpec(memory_space=pltpu.VMEM)] * 7 + [pl.BlockSpec(memory_space=pl.ANY)] * 4,
        out_specs=[pl.BlockSpec(memory_space=pltpu.VMEM)] * 5,
        scratch_shapes=[
            vmem((32, 8, 3072), BF16),
            vmem((64, 8, 3072), BF16), vmem((64, 8, 3072), BF16),
            vmem((rows, D), BF16), vmem((rows, D), BF16),
            vmem((rows, hidden), BF16), vmem((rows, hidden), BF16), vmem((rows, hidden), BF16),
            slots, slots, slots, slots,
            vmem((9, 256, 128), BF16), vmem((64, 128), BF16), vmem((64, 128), BF16),
            vmem((4, 4, 4, 32, HALF), BF16), vmem((4, 128, HALF), BF16),
            vmem((128, 128), F32), vmem((128, 128), F32), vmem((128, 128), F32),
            vmem((4, 128, 512), BF16), vmem((4, 128, 512), BF16),
            vmem((16, 32, HALF), BF16), vmem((16, 32, HALF), BF16),
            vmem((160, HALF), F32),
            vmem((128, 128), F32), vmem((128, 128), F32), vmem((32, HALF), F32),
            dma((4,)), dma((32,)), dma((32,)), dma((64,)), dma((64,)), dma((64,)),
            dma((4,)), dma((4,)), dma((64,)), dma((64,)),
            dma((8, 3)), dma((8, 3)), dma, dma, dma((3,)), dma((3,)),
            dma, dma, dma((2, 2)), dma((4,)), dma((16,)), dma((16,)), dma, dma, dma, dma,
        ],
        compiler_params=pltpu.CompilerParams(
            collective_id=0, has_side_effects=True, vmem_limit_bytes=VMEM_BYTES
        ),
        name="layer",
    )(
        routes.T, route_probs.T, stream_mid, out_grad, conv_out, ln_gain[None, :], taps,
        gate_slabs[0], up_slabs[0], down_slabs[0], proj_weight,
    )
    return grad_input, grad_proj, grad_gate[None], grad_up[None], grad_down[None]


def solution(mesh):
    return jax.shard_map(
        on_device,
        mesh=mesh,
        in_specs=(
            P("sp", "tp"), P("tp"), P(None, "tp"), P("sp", "tp"), P("sp", "tp"), P("sp", "tp"),
            P("sp", None), P("sp", None), P("sp", None, "tp"), P("sp", None, "tp"), P("sp", "tp", None),
        ),
        out_specs=(
            P("sp", "tp"), P("sp", "tp"), P("sp", None, "tp"), P("sp", None, "tp"), P("sp", "tp", None),
        ),
        check_vma=False,
    )
```

```python
import functools

import jax
import jax.numpy as jnp
from jax import lax
from jax.experimental import pallas as pl
from jax.experimental.pallas import tpu as pltpu
from jax.sharding import PartitionSpec as P

D = 2048
HALF = 1024
MAIN = 8
REM = 4
MESH = pl.DeviceIdType.MESH
F32 = jnp.float32
BF16 = jnp.bfloat16
VMEM_BYTES = 42 * 1024 * 1024


def nt(a, b):
    return lax.dot_general(a, b, (((1,), (1,)), ((), ())), preferred_element_type=F32)


def nn(a, b):
    return lax.dot_general(a, b, (((1,), (0,)), ((), ())), preferred_element_type=F32)


def tn(a, b):
    return lax.dot_general(a, b, (((0,), (0,)), ((), ())), preferred_element_type=F32)


def sp_copy(src, dst, send, recv, sp):
    return pltpu.make_async_remote_copy(
        src_ref=src, dst_ref=dst, send_sem=send, recv_sem=recv,
        device_id={"sp": sp}, device_id_type=MESH,
    )


def tp_copy(src, dst, send, recv, tp):
    return pltpu.make_async_remote_copy(
        src_ref=src, dst_ref=dst, send_sem=send, recv_sem=recv,
        device_id={"tp": tp}, device_id_type=MESH,
    )


def gray(k):
    return lax.rem(k + k // 2 - 2 * (k // 3), 4)


def layer_kernel(
    routes_hbm, probs_hbm, stream_hbm, out_grad_hbm, conv_hbm, gain_hbm, taps_hbm,
    wg_hbm, wu_hbm, wd_hbm, proj_hbm,
    gin_out, gproj_out, wg, wu, wd,
    routes, probs, stream, out_grad, conv, gain, taps,
    pk, own, oth, xs, ps, acts, dgs, dus, psend, precv, pown, ret,
    table, sel_a, sel_b, proj, act, stat_send, stat_recv, stats,
    gs, gz, part, parts, ext, sum_send, sum_recv, taps_f,
    w_sem, a_send, b_send, c_send, own_sem, oth_sem,
    e_send, e_recv, r_send, r_recv,
    g_send, g_recv, s_send, s_recv, t_send, t_recv,
    i_sem, q_send, q_recv, z_send, z_recv, p_send, p_recv, u_send, u_recv, h_send, h_recv,
):
    me = lax.axis_index("sp")
    tp = lax.axis_index("tp")
    peer = 1 - tp
    mx, my, mz = lax.rem(me, 4), lax.rem(me // 4, 4), me // 16
    here = lax.rem(me, 16)
    twin = me + 1 - 2 * lax.rem(me, 2)
    loads = [
        pltpu.make_async_copy(src, dst, w_sem.at[i])
        for i, (src, dst) in enumerate(((wg_hbm, wg), (wu_hbm, wu), (wd_hbm, wd)))
    ]
    small = [
        pltpu.make_async_copy(src, dst, i_sem.at[i])
        for i, (src, dst) in enumerate(
            (
                (routes_hbm, routes), (probs_hbm, probs), (stream_hbm, stream),
                (out_grad_hbm, out_grad), (conv_hbm, conv), (gain_hbm, gain), (taps_hbm, taps),
            )
        )
    ]
    for copy in small:
        copy.start()
    proj_load = pltpu.make_async_copy(proj_hbm, proj.at[mz, my, mx], w_sem.at[3])
    proj_load.start()
    for copy in loads:
        copy.start()

    barrier = pltpu.get_barrier_semaphore()

    def greet(k, _):
        pl.semaphore_signal(
            barrier, inc=1, device_id={"sp": lax.rem(me + k, 64)}, device_id_type=MESH
        )
        return 0

    lax.fori_loop(1, 64, greet, 0)
    pl.semaphore_signal(barrier, inc=1, device_id={"tp": peer}, device_id_type=MESH)
    for d in (1, 2, 3):
        pl.semaphore_signal(
            barrier, inc=1, device_id={"sp": lax.rem(mz + d, 4) * 16 + here, "tp": peer},
            device_id_type=MESH,
        )

    for copy in small:
        copy.wait()

    expert = lax.broadcasted_iota(jnp.int32, (128, 128), 0)
    other = lax.broadcasted_iota(jnp.int32, (128, 128), 1)
    picks = [expert == routes[j : j + 1, :] for j in range(2)]
    counts = picks[0].astype(F32) + picks[1].astype(F32)
    before = nn(counts.astype(BF16), (expert < other).astype(F32).astype(BF16))
    at = lax.broadcasted_iota(jnp.int32, (256, 128), 0)
    for j in range(2):
        slot_row = jnp.sum(jnp.where(picks[j], before, 0.0), axis=0, keepdims=True)
        slot_row = slot_row.astype(jnp.int32)
        base = routes[j : j + 1, :] * MAIN + slot_row
        near = jnp.where(slot_row < MAIN, base, -1)
        far = jnp.where(slot_row < MAIN, -1, base)
        table[3 * j] = (at == near).astype(F32).astype(BF16)
        table[3 * j + 1] = (at + MAIN == far).astype(F32).astype(BF16)
        table[3 * j + 2] = (at + REM == far).astype(F32).astype(BF16)
    for i in range(3):
        table[6 + i] = table[i] + table[3 + i]
    shape = (32, 8, HALF)
    pk[:, :, :HALF] = nn(table[6], stream[...]).astype(BF16).reshape(shape)
    rest = nn(table[7], stream[:, :512]) + nn(table[8], stream[:, 512:])
    pk[:, :, 2 * HALF : 2 * HALF + 512] = rest.astype(BF16).reshape(32, 8, 512)
    grads = []
    for j in range(2):
        prob = jnp.broadcast_to(probs[j : j + 1, :], (128, 128)).T[:, 0:1]
        grads.append((out_grad[...].astype(F32) * prob).astype(BF16))
    near = nn(table[0], grads[0]) + nn(table[3], grads[1])
    pk[:, :, HALF : 2 * HALF] = near.astype(BF16).reshape(shape)
    rest = nn(table[1], grads[0][:, :512]) + nn(table[4], grads[1][:, :512])
    rest = rest + nn(table[2], grads[0][:, 512:]) + nn(table[5], grads[1][:, 512:])
    pk[:, :, 2 * HALF + 512 :] = rest.astype(BF16).reshape(32, 8, 512)

    row = lax.broadcasted_iota(jnp.int32, (64, 128), 0)
    col = lax.broadcasted_iota(jnp.int32, (64, 128), 1)
    spot = (row // 4) * 8 + row % 4
    sel_a[...] = (col == spot).astype(F32).astype(BF16)
    sel_b[...] = (col == spot + 4).astype(F32).astype(BF16)
    own[pl.ds(me, 1)] = pk[pl.ds(me // 2, 1)]
    values = conv[...].astype(F32)
    lane = lax.broadcasted_iota(jnp.int32, (128, 128), 1)
    total = jnp.sum(values, axis=1, keepdims=True)
    squares = jnp.sum(values * values, axis=1, keepdims=True)
    stat_send[...] = jnp.where(lane == 0, total, squares)
    proj_load.wait()

    pl.semaphore_wait(barrier, 67)

    def direct_send(i):
        k, j = i // 8, lax.rem(i, 8)
        dz, dy, side = gray(k), gray(j // 2), lax.rem(j, 2)
        x = mx + side * (3 - 2 * mx)
        to = lax.rem(mz + dz, 4) * 16 + lax.rem(my + dy, 4) * 4 + x
        return sp_copy(pk.at[to // 2], own.at[me], a_send.at[i], own_sem.at[me], to)

    def start_direct(i, _):
        direct_send(i).start()
        return 0

    stat_copy = tp_copy(stat_send, stat_recv, s_send, s_recv, peer)
    stat_copy.start()

    def gather(group, axis, part):
        def at(d):
            z, y, x = mz, my, mx
            if axis == 0:
                z = lax.rem(mz + d, 4)
            elif axis == 1:
                y = lax.rem(my + d, 4)
            else:
                x = lax.rem(mx + d, 4)
            return z, y, x

        def copy(d, send):
            z, y, x = at(0) if send else at(4 - d)
            to_z, to_y, to_x = at(d)
            block = proj.at[part(z, y, x)]
            return sp_copy(
                block, block, g_send.at[group, d - 1], g_recv.at[group, d - 1],
                to_z * 16 + to_y * 4 + to_x,
            )

        def start():
            for d in (1, 3, 2):
                copy(d, True).start()

        def take():
            for d in (1, 3, 2):
                copy(d, False).wait_recv()

        def sent():
            for d in (1, 3, 2):
                copy(d, True).wait_send()

        return start, take, sent

    every = slice(None)
    low, mid_cols, high = pl.ds(0, 256), pl.ds(256, 512), pl.ds(768, 256)
    first_hop = (
        gather(0, 2, lambda z, y, x: (z, y, x, every, pl.ds(0, 768))),
        gather(1, 1, lambda z, y, x: (z, y, x, every, high)),
    )
    second_hop = (
        gather(2, 1, lambda z, y, x: (z, y, every, every, low)),
        gather(3, 0, lambda z, y, x: (z, y, every, every, mid_cols)),
        gather(4, 0, lambda z, y, x: (z, every, x, every, high)),
    )
    third_hop = (
        gather(5, 0, lambda z, y, x: (z, every, every, every, low)),
        gather(6, 1, lambda z, y, x: (every, y, every, every, mid_cols)),
        gather(7, 2, lambda z, y, x: (every, every, x, every, high)),
    )
    for start, _, _ in first_hop:
        start()
    lax.fori_loop(1, 32, start_direct, 0)

    stat_copy.wait_recv()
    both = stat_send[...] + stat_recv[...]
    row_mean = both[:, 0:1] / D
    row_var = both[:, 1:2] / D - row_mean * row_mean
    inv_std = lax.rsqrt(row_var + 1e-06)
    stats[...] = jnp.where(lane == 0, row_mean, inv_std)
    scaled_z = (values - row_mean) * inv_std * gain[...]
    act[pl.ds(mz, 1)] = (scaled_z * jax.nn.sigmoid(scaled_z)).astype(BF16)[None]

    def act_copy(d, send):
        z = mz if send else lax.rem(mz + 4 - d, 4)
        return sp_copy(
            act.at[z], act.at[z], t_send.at[d - 1], t_recv.at[d - 1],
            lax.rem(mz + d, 4) * 16 + lax.rem(me, 16),
        )

    def source(k, j, near):
        dz, dy, side = gray(k), gray(j // 2), lax.rem(j, 2)
        x = mx + side * (3 - 2 * mx)
        twin_x = x + 1 - 2 * lax.rem(x, 2)
        x = x if near else twin_x
        return lax.rem(mz - dz + 4, 4) * 16 + lax.rem(my - dy + 4, 4) * 4 + x

    def twin_copy(i):
        s = source(i // 8, lax.rem(i, 8), True)
        return sp_copy(own.at[s], own.at[s], b_send.at[i], own_sem.at[s], twin)

    def core_copy(s):
        return tp_copy(own.at[s], oth.at[s], c_send.at[s], oth_sem.at[s], peer)

    def arrived(s):
        return sp_copy(own.at[s], own.at[s], c_send.at[s], own_sem.at[s], twin)

    def take_direct(k):
        def one(j, _):
            s = source(k, j, True)

            @pl.when(k * 8 + j != 0)
            def _():
                arrived(s).wait_recv()

            twin_copy(k * 8 + j).start()
            core_copy(s).start()
            return 0

        lax.fori_loop(0, 8, one, 0)

    def take_twin(k):
        def one(j, _):
            s = source(k, j, False)
            arrived(s).wait_recv()
            core_copy(s).start()
            return 0

        lax.fori_loop(0, 8, one, 0)

    def part_copy(z):
        return tp_copy(
            psend.at[pl.ds(z * 16, 16)], precv.at[pl.ds(z * 16, 16)],
            e_send.at[z], e_recv.at[z], peer,
        )

    def slot(s):
        return lax.rem(s, 2) * 32 + s // 2

    def ret_copy(s):
        return sp_copy(pown.at[s], ret.at[slot(me)], r_send.at[s], r_recv.at[me], s)

    def ret_arrived(s):
        return sp_copy(pown.at[s], ret.at[slot(s)], r_send.at[s], r_recv.at[s], s)

    def plane(k):
        return lax.rem(mz - gray(k) + 4, 4)

    def compute(k):
        z = plane(k)

        def wait_other(j, _):
            tp_copy(
                own.at[z * 16 + j], oth.at[z * 16 + j],
                c_send.at[z * 16 + j], oth_sem.at[z * 16 + j], peer,
            ).wait_recv()
            return 0

        lax.fori_loop(0, 16, wait_other, 0)
        base = pl.multiple_of(z * 192, 64)
        for buf, half in ((own, tp), (oth, peer)):
            block = buf[pl.ds(z * 16, 16)].reshape(128, 3072)
            left = pl.multiple_of(half * HALF, HALF)
            mid = pl.multiple_of(half * HALF + 512, 512)
            xs[pl.ds(base, 128), pl.ds(left, HALF)] = block[:, :HALF]
            ps[pl.ds(base, 128), pl.ds(left, HALF)] = block[:, HALF : 2 * HALF]
            rest = block[:, 2 * HALF :]
            first = nn(sel_a[...], rest).astype(BF16)
            second = nn(sel_b[...], rest).astype(BF16)
            low = pl.multiple_of(base + 128, 64)
            xs[pl.ds(low, 64), pl.ds(left, 512)] = first[:, :512]
            xs[pl.ds(low, 64), pl.ds(mid, 512)] = second[:, :512]
            ps[pl.ds(low, 64), pl.ds(left, 512)] = first[:, 512:]
            ps[pl.ds(low, 64), pl.ds(mid, 512)] = second[:, 512:]
        x = xs[pl.ds(base, 192), :]
        p = ps[pl.ds(base, 192), :]
        g = nn(x, wg[...])
        u = nn(x, wu[...])
        dh = nt(p, wd[...])
        sig = jax.nn.sigmoid(g)
        silu = g * sig
        acts[pl.ds(base, 192), :] = (silu * u).astype(BF16)
        dg = (dh * u * sig * (1.0 + g * (1.0 - sig))).astype(BF16)
        du = (dh * silu).astype(BF16)
        dgs[pl.ds(base, 192), :] = dg
        dus[pl.ds(base, 192), :] = du
        for out, half in ((psend, peer), (pown, tp)):
            rows = pl.ds(pl.multiple_of(half * HALF, HALF), HALF)
            back = nt(dg, wg[rows, :]) + nt(du, wu[rows, :])
            back = back.astype(BF16)
            out[pl.ds(z * 16, 16), :, :HALF] = back[:128].reshape(16, 8, HALF)
            rest = tn(sel_a[...], back[128:, :512]) + tn(sel_b[...], back[128:, 512:])
            out[pl.ds(z * 16, 16), :, HALF:] = rest.astype(BF16).reshape(16, 8, 512)
            if half is peer:
                part_copy(z).start()

    def give_back(k):
        z = plane(k)
        part_copy(z).wait_recv()
        block = pl.ds(z * 16, 16)
        pown[block] = (pown[block].astype(F32) + precv[block].astype(F32)).astype(BF16)

        def one(j, _):
            s = z * 16 + lax.rem(lax.rem(me, 16) + j, 16)

            @pl.when(s != me)
            def _():
                ret_copy(s).start()

            return 0

        lax.fori_loop(0, 16, one, 0)

    for _, take, _ in first_hop:
        take()
    for start, _, _ in second_hop:
        start()
    take_direct(0)
    for d in (1, 3, 2):
        act_copy(d, True).start()
    take_direct(1)
    for _, take, _ in second_hop:
        take()
    for start, _, _ in third_hop[:2]:
        start()
    take_twin(0)
    for copy in loads:
        copy.wait()

    def step(k, _):
        @pl.when(k < 2)
        def _():
            take_direct(k + 2)

        @pl.when(k > 0)
        def _():
            give_back(k - 1)

        compute(k)

        @pl.when(k < 3)
        def _():
            take_twin(k + 1)


        return 0

    lax.fori_loop(0, 4, step, 0)
    give_back(3)
    ret[pl.ds(slot(me), 1)] = pown[pl.ds(me, 1)]
    third_hop[2][0]()

    def weight_grads(i, _):
        cols = pl.ds(pl.multiple_of(i * 256, 256), 256)
        rows = xs[:, cols].T
        wg[cols, :] = nn(rows, dgs[...]).astype(BF16)
        wu[cols, :] = nn(rows, dus[...]).astype(BF16)
        return 0

    lax.fori_loop(0, 8, weight_grads, 0)

    def down_grads(i, _):
        cols = pl.ds(pl.multiple_of(i * 128, 128), 128)
        wd[cols, :] = nn(acts[:, cols].T, ps[...]).astype(BF16)
        return 0

    lax.fori_loop(0, 7, down_grads, 0)
    taps_f[pl.ds(0, 31), :] = taps[...].astype(F32)

    def await_return(s, _):
        @pl.when(s != me)
        def _():
            ret_arrived(s).wait_recv()

        return 0

    lax.fori_loop(0, 64, await_return, 0)
    contrib = jnp.zeros((128, HALF), F32)
    halves = []
    for h in range(2):
        block = ret[pl.ds(h * 32, 32)].reshape(256, 1536)
        contrib = contrib + tn(table[6], block[:, :HALF])
        halves.append(block[:, HALF:])
    left = tn(table[7], halves[0]) + tn(table[7], halves[1])
    right = tn(table[8], halves[0]) + tn(table[8], halves[1])
    left = (out_grad[:, :512].astype(F32) + (contrib[:, :512] + left)).astype(BF16)
    right = (out_grad[:, 512:].astype(F32) + (contrib[:, 512:] + right)).astype(BF16)
    gs[pl.ds(2 * tp, 1)] = left[None]
    gs[pl.ds(2 * tp + 1, 1)] = right[None]

    def stream_copy(tp_of):
        rows = pl.ds(2 * tp_of, 2)
        return tp_copy(gs.at[rows], gs.at[rows], q_send, q_recv, peer)

    def plane_copy(z, core, i):
        return pltpu.make_async_remote_copy(
            src_ref=gs.at[z], dst_ref=gz.at[mz],
            send_sem=z_send.at[i, core], recv_sem=z_recv.at[mz],
            device_id={"sp": z * 16 + here, "tp": core}, device_id_type=MESH,
        )

    def plane_arrived(z):
        return sp_copy(gz.at[z], gz.at[z], z_send.at[0, 0], z_recv.at[z], z * 16 + here)

    stream_copy(tp).start()
    for i in range(2):
        z = 2 * tp + i

        @pl.when(z != mz)
        def _():
            plane_copy(z, 0, i).start()
            plane_copy(z, 1, i).start()

    for d in (1, 2, 3):
        act_copy(d, False).wait_recv()

    def weights(z):
        return proj[pl.ds(z, 1)].reshape(512, HALF)

    for _, take, _ in third_hop:
        take()
    grad_act = nn(left, weights(2 * tp)) + nn(right, weights(2 * tp + 1))
    stream_copy(peer).wait_recv()
    mine = gs[pl.ds(mz, 1)].reshape(128, 512)
    total = tn(mine, act[pl.ds(mz, 1)].reshape(128, HALF))
    for d in (1, 3, 2):
        z = lax.rem(mz + d, 4)
        plane_arrived(z).wait_recv()
        total = total + tn(gz[pl.ds(z, 1)].reshape(128, 512), act[pl.ds(z, 1)].reshape(128, HALF))
    part[...] = total.astype(BF16).reshape(16, 32, HALF)

    def proj_copy(d):
        q = lax.rem(here + d, 16)
        return sp_copy(part.at[q], parts.at[here], p_send.at[d], p_recv.at[here], mz * 16 + q)

    def part_arrived(q):
        return sp_copy(parts.at[q], parts.at[q], p_send.at[0], p_recv.at[q], mz * 16 + q)

    def start_part(d, _):
        proj_copy(d).start()
        return 0

    other = gs[pl.ds(2 * peer, 2)]
    grad_act = grad_act + nn(other[0], weights(2 * peer)) + nn(other[1], weights(2 * peer + 1))
    lax.fori_loop(1, 16, start_part, 0)

    row_mean, inv_std = stats[:, 0:1], stats[:, 1:2]
    normed = (conv[...].astype(F32) - row_mean) * inv_std
    scaled_z = normed * gain[...]
    z_sig = jax.nn.sigmoid(scaled_z)
    grad_normed = grad_act * z_sig * (1.0 + scaled_z * (1.0 - z_sig)) * gain[...]
    sum_send[...] = jnp.where(
        lane == 0,
        jnp.sum(grad_normed, axis=1, keepdims=True),
        jnp.sum(grad_normed * normed, axis=1, keepdims=True),
    )
    sum_copy = tp_copy(sum_send, sum_recv, u_send, u_recv, peer)
    sum_copy.start()
    sum_copy.wait_recv()
    both = sum_send[...] + sum_recv[...]
    grad_conv = inv_std * (grad_normed - both[:, 0:1] / D - normed * (both[:, 1:2] / D))
    ext[pl.ds(0, 128), :] = grad_conv.astype(BF16).astype(F32)

    def reach_copy(to):
        return sp_copy(ext.at[pl.ds(0, 32)], ext.at[pl.ds(128, 32)], h_send, h_recv, to)

    @pl.when(me == 63)
    def _():
        ext[pl.ds(128, 32), :] = jnp.zeros((32, HALF), F32)

    @pl.when(me > 0)
    def _():
        reach_copy(me - 1).start()

    parts[pl.ds(here, 1)] = part[pl.ds(here, 1)]

    @pl.when(me < 63)
    def _():
        reach_copy(me + 1).wait_recv()

    def columns(c, _):
        cols = pl.ds(pl.multiple_of(c * 128, 128), 128)
        acc = jnp.zeros((128, 128), F32)
        for k in range(31):
            acc = acc + taps_f[pl.ds(k, 1), cols] * ext[pl.ds(k, 128), cols]
        gin_out[:, cols] = acc.astype(BF16)
        return 0

    lax.fori_loop(0, 8, columns, 0)

    def wait_part(d, _):
        part_arrived(lax.rem(here + d, 16)).wait_recv()
        return 0

    lax.fori_loop(1, 16, wait_part, 0)
    result = parts[0].astype(F32)
    for q in range(1, 16):
        result = result + parts[q].astype(F32)
    gproj_out[...] = result

    def sent_part(d, _):
        proj_copy(d).wait_send()
        return 0

    lax.fori_loop(1, 16, sent_part, 0)
    stream_copy(tp).wait_send()
    sum_copy.wait_send()
    for i in range(2):
        z = 2 * tp + i

        @pl.when(z != mz)
        def _():
            plane_copy(z, 0, i).wait_send()
            plane_copy(z, 1, i).wait_send()

    @pl.when(me > 0)
    def _():
        reach_copy(me - 1).wait_send()

    def finish_sends(i, _):
        @pl.when(i > 0)
        def _():
            direct_send(i).wait_send()

        twin_copy(i).wait_send()
        return 0

    lax.fori_loop(0, 32, finish_sends, 0)

    def finish(s, _):
        core_copy(s).wait_send()

        @pl.when(s != me)
        def _():
            ret_copy(s).wait_send()

        return 0

    lax.fori_loop(0, 64, finish, 0)
    for z in range(4):
        part_copy(z).wait_send()
    for _, _, sent in first_hop + second_hop + third_hop:
        sent()
    for d in (1, 2, 3):
        act_copy(d, True).wait_send()
    stat_copy.wait_send()
def on_device(
    conv_out, ln_gain, taps, proj_weight, stream_mid, out_grad,
    routes, route_probs, gate_slabs, up_slabs, down_slabs,
):
    hidden = gate_slabs.shape[2]
    rows = 768
    dma = pltpu.SemaphoreType.DMA
    vmem = pltpu.VMEM
    slots = vmem((64, 8, 1536), BF16)
    grad_input, grad_proj, grad_gate, grad_up, grad_down = pl.pallas_call(
        layer_kernel,
        out_shape=[
            jax.ShapeDtypeStruct((128, HALF), BF16),
            jax.ShapeDtypeStruct((32, HALF), F32),
            jax.ShapeDtypeStruct((D, hidden), BF16),
            jax.ShapeDtypeStruct((D, hidden), BF16),
            jax.ShapeDtypeStruct((hidden, D), BF16),
        ],
        in_specs=[pl.BlockSpec(memory_space=pl.ANY)] * 11,
        out_specs=[pl.BlockSpec(memory_space=pltpu.VMEM)] * 5,
        scratch_shapes=[
            vmem((2, 128), jnp.int32), vmem((2, 128), F32),
            vmem((128, HALF), BF16), vmem((128, HALF), BF16), vmem((128, HALF), BF16),
            vmem((1, HALF), F32), vmem((31, HALF), BF16),
            vmem((32, 8, 3072), BF16),
            vmem((64, 8, 3072), BF16), vmem((64, 8, 3072), BF16),
            vmem((rows, D), BF16), vmem((rows, D), BF16),
            vmem((rows, hidden), BF16), vmem((rows, hidden), BF16), vmem((rows, hidden), BF16),
            slots, slots, slots, slots,
            vmem((9, 256, 128), BF16), vmem((64, 128), BF16), vmem((64, 128), BF16),
            vmem((4, 4, 4, 32, HALF), BF16), vmem((4, 128, HALF), BF16),
            vmem((128, 128), F32), vmem((128, 128), F32), vmem((128, 128), F32),
            vmem((4, 128, 512), BF16), vmem((4, 128, 512), BF16),
            vmem((16, 32, HALF), BF16), vmem((16, 32, HALF), BF16),
            vmem((160, HALF), F32),
            vmem((128, 128), F32), vmem((128, 128), F32), vmem((32, HALF), F32),
            dma((4,)), dma((32,)), dma((32,)), dma((64,)), dma((64,)), dma((64,)),
            dma((4,)), dma((4,)), dma((64,)), dma((64,)),
            dma((8, 3)), dma((8, 3)), dma, dma, dma((3,)), dma((3,)),
            dma((7,)), dma, dma, dma((2, 2)), dma((4,)), dma((16,)), dma((16,)), dma, dma, dma, dma,
        ],
        compiler_params=pltpu.CompilerParams(
            collective_id=0, has_side_effects=True, vmem_limit_bytes=VMEM_BYTES
        ),
        name="layer",
    )(
        *(
            pltpu.with_memory_space_constraint(a, pltpu.HBM)
            for a in (
                routes.T, route_probs.T, stream_mid, out_grad, conv_out, ln_gain[None, :], taps,
                gate_slabs[0], up_slabs[0], down_slabs[0], proj_weight,
            )
        )
    )
    return grad_input, grad_proj, grad_gate[None], grad_up[None], grad_down[None]


def solution(mesh):
    return jax.shard_map(
        on_device,
        mesh=mesh,
        in_specs=(
            P("sp", "tp"), P("tp"), P(None, "tp"), P("sp", "tp"), P("sp", "tp"), P("sp", "tp"),
            P("sp", None), P("sp", None), P("sp", None, "tp"), P("sp", None, "tp"), P("sp", "tp", None),
        ),
        out_specs=(
            P("sp", "tp"), P("sp", "tp"), P("sp", None, "tp"), P("sp", None, "tp"), P("sp", "tp", None),
        ),
        check_vma=False,
    )
```

```python
import functools

import jax
import jax.numpy as jnp
from jax import lax
from jax.experimental import pallas as pl
from jax.experimental.pallas import tpu as pltpu
from jax.sharding import PartitionSpec as P

D = 2048
HALF = 1024
MAIN = 8
REM = 4
MESH = pl.DeviceIdType.MESH
F32 = jnp.float32
BF16 = jnp.bfloat16
VMEM_BYTES = 42 * 1024 * 1024


def nt(a, b):
    return lax.dot_general(a, b, (((1,), (1,)), ((), ())), preferred_element_type=F32)


def nn(a, b):
    return lax.dot_general(a, b, (((1,), (0,)), ((), ())), preferred_element_type=F32)


def tn(a, b):
    return lax.dot_general(a, b, (((0,), (0,)), ((), ())), preferred_element_type=F32)


def sp_copy(src, dst, send, recv, sp):
    return pltpu.make_async_remote_copy(
        src_ref=src, dst_ref=dst, send_sem=send, recv_sem=recv,
        device_id={"sp": sp}, device_id_type=MESH,
    )


def tp_copy(src, dst, send, recv, tp):
    return pltpu.make_async_remote_copy(
        src_ref=src, dst_ref=dst, send_sem=send, recv_sem=recv,
        device_id={"tp": tp}, device_id_type=MESH,
    )


def gray(k):
    return lax.rem(k + k // 2 - 2 * (k // 3), 4)


def layer_kernel(
    routes_hbm, probs_hbm, stream_hbm, out_grad_hbm, conv_hbm, gain_hbm, taps_hbm,
    wg_hbm, wu_hbm, wd_hbm, proj_hbm,
    gin_out, gproj_out, wg, wu, wd,
    routes, probs, stream, out_grad, conv, gain, taps,
    pk, own, oth, xs, ps, acts, dgs, dus, psend, precv, pown, ret,
    table, sel_a, sel_b, proj, act, stat_send, stat_recv, stats,
    gs, gz, part, parts, ext, sum_send, sum_recv, taps_f,
    w_sem, a_send, b_send, c_send, own_sem, oth_sem,
    e_send, e_recv, r_send, r_recv,
    g_send, g_recv, s_send, s_recv, t_send, t_recv,
    i_sem, q_send, q_recv, z_send, z_recv, p_send, p_recv, u_send, u_recv, h_send, h_recv,
):
    me = lax.axis_index("sp")
    tp = lax.axis_index("tp")
    peer = 1 - tp
    mx, my, mz = lax.rem(me, 4), lax.rem(me // 4, 4), me // 16
    here = lax.rem(me, 16)
    twin = me + 1 - 2 * lax.rem(me, 2)
    loads = [
        pltpu.make_async_copy(src, dst, w_sem.at[i])
        for i, (src, dst) in enumerate(((wg_hbm, wg), (wu_hbm, wu), (wd_hbm, wd)))
    ]
    small = [
        pltpu.make_async_copy(src, dst, i_sem.at[i])
        for i, (src, dst) in enumerate(
            (
                (routes_hbm, routes), (probs_hbm, probs), (stream_hbm, stream),
                (out_grad_hbm, out_grad), (conv_hbm, conv), (gain_hbm, gain), (taps_hbm, taps),
            )
        )
    ]
    for copy in small:
        copy.start()
    proj_load = pltpu.make_async_copy(proj_hbm, proj.at[mz, my, mx], w_sem.at[3])
    proj_load.start()
    for copy in loads:
        copy.start()

    barrier = pltpu.get_barrier_semaphore()

    def greet(k, _):
        pl.semaphore_signal(
            barrier, inc=1, device_id={"sp": lax.rem(me + k, 64)}, device_id_type=MESH
        )
        return 0

    lax.fori_loop(1, 64, greet, 0)
    pl.semaphore_signal(barrier, inc=1, device_id={"tp": peer}, device_id_type=MESH)
    for d in (1, 2, 3):
        pl.semaphore_signal(
            barrier, inc=1, device_id={"sp": lax.rem(mz + d, 4) * 16 + here, "tp": peer},
            device_id_type=MESH,
        )

    for copy in small:
        copy.wait()

    expert = lax.broadcasted_iota(jnp.int32, (128, 128), 0)
    other = lax.broadcasted_iota(jnp.int32, (128, 128), 1)
    picks = [expert == routes[j : j + 1, :] for j in range(2)]
    counts = picks[0].astype(F32) + picks[1].astype(F32)
    before = nn(counts.astype(BF16), (expert < other).astype(F32).astype(BF16))
    at = lax.broadcasted_iota(jnp.int32, (256, 128), 0)
    for j in range(2):
        slot_row = jnp.sum(jnp.where(picks[j], before, 0.0), axis=0, keepdims=True)
        slot_row = slot_row.astype(jnp.int32)
        base = routes[j : j + 1, :] * MAIN + slot_row
        near = jnp.where(slot_row < MAIN, base, -1)
        far = jnp.where(slot_row < MAIN, -1, base)
        table[3 * j] = (at == near).astype(F32).astype(BF16)
        table[3 * j + 1] = (at + MAIN == far).astype(F32).astype(BF16)
        table[3 * j + 2] = (at + REM == far).astype(F32).astype(BF16)
    for i in range(3):
        table[6 + i] = table[i] + table[3 + i]
    shape = (32, 8, HALF)
    pk[:, :, :HALF] = nn(table[6], stream[...]).astype(BF16).reshape(shape)
    rest = nn(table[7], stream[:, :512]) + nn(table[8], stream[:, 512:])
    pk[:, :, 2 * HALF : 2 * HALF + 512] = rest.astype(BF16).reshape(32, 8, 512)
    p_main = table[0].astype(F32) * probs[0:1, :] + table[3].astype(F32) * probs[1:2, :]
    p_main = jnp.sum(p_main, axis=1, keepdims=True)
    near = nn(table[6], out_grad[...]) * p_main
    pk[:, :, HALF : 2 * HALF] = near.astype(BF16).reshape(shape)
    p_rest = (table[1] + table[2]).astype(F32) * probs[0:1, :]
    p_rest = p_rest + (table[4] + table[5]).astype(F32) * probs[1:2, :]
    p_rest = jnp.sum(p_rest, axis=1, keepdims=True)
    rest = nn(table[7], out_grad[:, :512]) + nn(table[8], out_grad[:, 512:])
    pk[:, :, 2 * HALF + 512 :] = (rest * p_rest).astype(BF16).reshape(32, 8, 512)

    proj_load.wait()

    pl.semaphore_wait(barrier, 67)

    def direct_send(i):
        k, j = i // 8, lax.rem(i, 8)
        dz, dy, side = gray(k), gray(j // 2), lax.rem(j, 2)
        x = mx + side * (3 - 2 * mx)
        to = lax.rem(mz + dz, 4) * 16 + lax.rem(my + dy, 4) * 4 + x
        return sp_copy(pk.at[to // 2], own.at[me], a_send.at[i], own_sem.at[me], to)

    def start_direct(i, _):
        direct_send(i).start()
        return 0


    def gather(group, axis, part):
        def at(d):
            z, y, x = mz, my, mx
            if axis == 0:
                z = lax.rem(mz + d, 4)
            elif axis == 1:
                y = lax.rem(my + d, 4)
            else:
                x = lax.rem(mx + d, 4)
            return z, y, x

        def copy(d, send):
            z, y, x = at(0) if send else at(4 - d)
            to_z, to_y, to_x = at(d)
            block = proj.at[part(z, y, x)]
            return sp_copy(
                block, block, g_send.at[group, d - 1], g_recv.at[group, d - 1],
                to_z * 16 + to_y * 4 + to_x,
            )

        def start():
            for d in (1, 3, 2):
                copy(d, True).start()

        def take():
            for d in (1, 3, 2):
                copy(d, False).wait_recv()

        def sent():
            for d in (1, 3, 2):
                copy(d, True).wait_send()

        return start, take, sent

    every = slice(None)
    low, mid_cols, high = pl.ds(0, 384), pl.ds(384, 512), pl.ds(896, 128)
    first_hop = (
        gather(0, 2, lambda z, y, x: (z, y, x, every, pl.ds(0, 896))),
        gather(1, 1, lambda z, y, x: (z, y, x, every, high)),
    )
    second_hop = (
        gather(2, 1, lambda z, y, x: (z, y, every, every, low)),
        gather(3, 0, lambda z, y, x: (z, y, every, every, mid_cols)),
        gather(4, 0, lambda z, y, x: (z, every, x, every, high)),
    )
    third_hop = (
        gather(5, 0, lambda z, y, x: (z, every, every, every, low)),
        gather(6, 1, lambda z, y, x: (every, y, every, every, mid_cols)),
        gather(7, 2, lambda z, y, x: (every, every, x, every, high)),
    )
    for start, _, _ in first_hop:
        start()
    lax.fori_loop(1, 32, start_direct, 0)

    row = lax.broadcasted_iota(jnp.int32, (64, 128), 0)
    col = lax.broadcasted_iota(jnp.int32, (64, 128), 1)
    spot = (row // 4) * 8 + row % 4
    sel_a[...] = (col == spot).astype(F32).astype(BF16)
    sel_b[...] = (col == spot + 4).astype(F32).astype(BF16)
    own[pl.ds(me, 1)] = pk[pl.ds(me // 2, 1)]
    values = conv[...].astype(F32)
    lane = lax.broadcasted_iota(jnp.int32, (128, 128), 1)
    total = jnp.sum(values, axis=1, keepdims=True)
    squares = jnp.sum(values * values, axis=1, keepdims=True)
    stat_send[...] = jnp.where(lane == 0, total, squares)
    stat_copy = tp_copy(stat_send, stat_recv, s_send, s_recv, peer)
    stat_copy.start()

    stat_copy.wait_recv()
    both = stat_send[...] + stat_recv[...]
    row_mean = both[:, 0:1] / D
    row_var = both[:, 1:2] / D - row_mean * row_mean
    inv_std = lax.rsqrt(row_var + 1e-06)
    stats[...] = jnp.where(lane == 0, row_mean, inv_std)
    scaled_z = (values - row_mean) * inv_std * gain[...]
    act[pl.ds(mz, 1)] = (scaled_z * jax.nn.sigmoid(scaled_z)).astype(BF16)[None]

    def act_copy(d, send):
        z = mz if send else lax.rem(mz + 4 - d, 4)
        return sp_copy(
            act.at[z], act.at[z], t_send.at[d - 1], t_recv.at[d - 1],
            lax.rem(mz + d, 4) * 16 + lax.rem(me, 16),
        )

    def source(k, j, near):
        dz, dy, side = gray(k), gray(j // 2), lax.rem(j, 2)
        x = mx + side * (3 - 2 * mx)
        twin_x = x + 1 - 2 * lax.rem(x, 2)
        x = x if near else twin_x
        return lax.rem(mz - dz + 4, 4) * 16 + lax.rem(my - dy + 4, 4) * 4 + x

    def twin_copy(i):
        s = source(i // 8, lax.rem(i, 8), True)
        return sp_copy(own.at[s], own.at[s], b_send.at[i], own_sem.at[s], twin)

    def core_copy(s):
        return tp_copy(own.at[s], oth.at[s], c_send.at[s], oth_sem.at[s], peer)

    def arrived(s):
        return sp_copy(own.at[s], own.at[s], c_send.at[s], own_sem.at[s], twin)

    def take_direct(k):
        def one(j, _):
            s = source(k, j, True)

            @pl.when(k * 8 + j != 0)
            def _():
                arrived(s).wait_recv()

            twin_copy(k * 8 + j).start()
            core_copy(s).start()
            return 0

        lax.fori_loop(0, 8, one, 0)

    def take_twin(k):
        def one(j, _):
            s = source(k, j, False)
            arrived(s).wait_recv()
            core_copy(s).start()
            return 0

        lax.fori_loop(0, 8, one, 0)

    def part_copy(z):
        return tp_copy(
            psend.at[pl.ds(z * 16, 16)], precv.at[pl.ds(z * 16, 16)],
            e_send.at[z], e_recv.at[z], peer,
        )

    def slot(s):
        return lax.rem(s, 2) * 32 + s // 2

    def ret_copy(s):
        return sp_copy(pown.at[s], ret.at[slot(me)], r_send.at[s], r_recv.at[me], s)

    def ret_arrived(s):
        return sp_copy(pown.at[s], ret.at[slot(s)], r_send.at[s], r_recv.at[s], s)

    def plane(k):
        return lax.rem(mz - gray(k) + 4, 4)

    def compute(k):
        z = plane(k)

        def wait_other(j, _):
            tp_copy(
                own.at[z * 16 + j], oth.at[z * 16 + j],
                c_send.at[z * 16 + j], oth_sem.at[z * 16 + j], peer,
            ).wait_recv()
            return 0

        lax.fori_loop(0, 16, wait_other, 0)
        base = pl.multiple_of(z * 192, 64)
        for buf, half in ((own, tp), (oth, peer)):
            block = buf[pl.ds(z * 16, 16)].reshape(128, 3072)
            left = pl.multiple_of(half * HALF, HALF)
            mid = pl.multiple_of(half * HALF + 512, 512)
            xs[pl.ds(base, 128), pl.ds(left, HALF)] = block[:, :HALF]
            ps[pl.ds(base, 128), pl.ds(left, HALF)] = block[:, HALF : 2 * HALF]
            rest = block[:, 2 * HALF :]
            first = nn(sel_a[...], rest).astype(BF16)
            second = nn(sel_b[...], rest).astype(BF16)
            low = pl.multiple_of(base + 128, 64)
            xs[pl.ds(low, 64), pl.ds(left, 512)] = first[:, :512]
            xs[pl.ds(low, 64), pl.ds(mid, 512)] = second[:, :512]
            ps[pl.ds(low, 64), pl.ds(left, 512)] = first[:, 512:]
            ps[pl.ds(low, 64), pl.ds(mid, 512)] = second[:, 512:]
        x = xs[pl.ds(base, 192), :]
        p = ps[pl.ds(base, 192), :]
        g = nn(x, wg[...])
        u = nn(x, wu[...])
        dh = nt(p, wd[...])
        sig = jax.nn.sigmoid(g)
        silu = g * sig
        acts[pl.ds(base, 192), :] = (silu * u).astype(BF16)
        dg = (dh * u * sig * (1.0 + g * (1.0 - sig))).astype(BF16)
        du = (dh * silu).astype(BF16)
        dgs[pl.ds(base, 192), :] = dg
        dus[pl.ds(base, 192), :] = du
        for out, half in ((psend, peer), (pown, tp)):
            rows = pl.ds(pl.multiple_of(half * HALF, HALF), HALF)
            back = nt(dg, wg[rows, :]) + nt(du, wu[rows, :])
            back = back.astype(BF16)
            out[pl.ds(z * 16, 16), :, :HALF] = back[:128].reshape(16, 8, HALF)
            rest = tn(sel_a[...], back[128:, :512]) + tn(sel_b[...], back[128:, 512:])
            out[pl.ds(z * 16, 16), :, HALF:] = rest.astype(BF16).reshape(16, 8, 512)
            if half is peer:
                part_copy(z).start()

    def give_back(k):
        z = plane(k)
        part_copy(z).wait_recv()
        block = pl.ds(z * 16, 16)
        pown[block] = (pown[block].astype(F32) + precv[block].astype(F32)).astype(BF16)

        def one(j, _):
            s = z * 16 + lax.rem(lax.rem(me, 16) + j, 16)

            @pl.when(s != me)
            def _():
                ret_copy(s).start()

            return 0

        lax.fori_loop(0, 16, one, 0)

    for _, take, _ in first_hop:
        take()
    for start, _, _ in second_hop:
        start()
    take_direct(0)
    for d in (1, 3, 2):
        act_copy(d, True).start()
    take_direct(1)
    for _, take, _ in second_hop:
        take()
    for start, _, _ in third_hop[:2]:
        start()
    take_twin(0)
    for copy in loads:
        copy.wait()

    def step(k, _):
        @pl.when(k < 2)
        def _():
            take_direct(k + 2)

        @pl.when(k > 0)
        def _():
            give_back(k - 1)

        compute(k)

        @pl.when(k < 3)
        def _():
            take_twin(k + 1)


        return 0

    lax.fori_loop(0, 4, step, 0)
    give_back(3)
    ret[pl.ds(slot(me), 1)] = pown[pl.ds(me, 1)]
    third_hop[2][0]()

    def weight_grads(i, _):
        cols = pl.ds(pl.multiple_of(i * 256, 256), 256)
        rows = xs[:, cols].T
        wg[cols, :] = nn(rows, dgs[...]).astype(BF16)
        wu[cols, :] = nn(rows, dus[...]).astype(BF16)
        return 0

    lax.fori_loop(0, 8, weight_grads, 0)

    def down_grads(i, _):
        cols = pl.ds(pl.multiple_of(i * 128, 128), 128)
        wd[cols, :] = nn(acts[:, cols].T, ps[...]).astype(BF16)
        return 0

    lax.fori_loop(0, 7, down_grads, 0)
    taps_f[pl.ds(0, 31), :] = taps[...].astype(F32)

    def await_return(s, _):
        @pl.when(s != me)
        def _():
            ret_arrived(s).wait_recv()

        return 0

    lax.fori_loop(0, 64, await_return, 0)
    contrib = jnp.zeros((128, HALF), F32)
    halves = []
    for h in range(2):
        block = ret[pl.ds(h * 32, 32)].reshape(256, 1536)
        contrib = contrib + tn(table[6], block[:, :HALF])
        halves.append(block[:, HALF:])
    left = tn(table[7], halves[0]) + tn(table[7], halves[1])
    right = tn(table[8], halves[0]) + tn(table[8], halves[1])
    left = (out_grad[:, :512].astype(F32) + (contrib[:, :512] + left)).astype(BF16)
    right = (out_grad[:, 512:].astype(F32) + (contrib[:, 512:] + right)).astype(BF16)
    gs[pl.ds(2 * tp, 1)] = left[None]
    gs[pl.ds(2 * tp + 1, 1)] = right[None]

    def stream_copy(tp_of):
        rows = pl.ds(2 * tp_of, 2)
        return tp_copy(gs.at[rows], gs.at[rows], q_send, q_recv, peer)

    def plane_copy(z, core, i):
        return pltpu.make_async_remote_copy(
            src_ref=gs.at[z], dst_ref=gz.at[mz],
            send_sem=z_send.at[i, core], recv_sem=z_recv.at[mz],
            device_id={"sp": z * 16 + here, "tp": core}, device_id_type=MESH,
        )

    def plane_arrived(z):
        return sp_copy(gz.at[z], gz.at[z], z_send.at[0, 0], z_recv.at[z], z * 16 + here)

    stream_copy(tp).start()
    for i in range(2):
        z = 2 * tp + i

        @pl.when(z != mz)
        def _():
            plane_copy(z, 0, i).start()
            plane_copy(z, 1, i).start()

    for d in (1, 2, 3):
        act_copy(d, False).wait_recv()

    def weights(z):
        return proj[pl.ds(z, 1)].reshape(512, HALF)

    for _, take, _ in third_hop:
        take()
    grad_act = nn(left, weights(2 * tp)) + nn(right, weights(2 * tp + 1))
    stream_copy(peer).wait_recv()
    mine = gs[pl.ds(mz, 1)].reshape(128, 512)
    total = tn(mine, act[pl.ds(mz, 1)].reshape(128, HALF))
    for d in (1, 3, 2):
        z = lax.rem(mz + d, 4)
        plane_arrived(z).wait_recv()
        total = total + tn(gz[pl.ds(z, 1)].reshape(128, 512), act[pl.ds(z, 1)].reshape(128, HALF))
    part[...] = total.astype(BF16).reshape(16, 32, HALF)

    def proj_copy(d):
        q = lax.rem(here + d, 16)
        return sp_copy(part.at[q], parts.at[here], p_send.at[d], p_recv.at[here], mz * 16 + q)

    def part_arrived(q):
        return sp_copy(parts.at[q], parts.at[q], p_send.at[0], p_recv.at[q], mz * 16 + q)

    def start_part(d, _):
        proj_copy(d).start()
        return 0

    other = gs[pl.ds(2 * peer, 2)]
    grad_act = grad_act + nn(other[0], weights(2 * peer)) + nn(other[1], weights(2 * peer + 1))
    lax.fori_loop(1, 16, start_part, 0)

    row_mean, inv_std = stats[:, 0:1], stats[:, 1:2]
    normed = (conv[...].astype(F32) - row_mean) * inv_std
    scaled_z = normed * gain[...]
    z_sig = jax.nn.sigmoid(scaled_z)
    grad_normed = grad_act * z_sig * (1.0 + scaled_z * (1.0 - z_sig)) * gain[...]
    sum_send[...] = jnp.where(
        lane == 0,
        jnp.sum(grad_normed, axis=1, keepdims=True),
        jnp.sum(grad_normed * normed, axis=1, keepdims=True),
    )
    sum_copy = tp_copy(sum_send, sum_recv, u_send, u_recv, peer)
    sum_copy.start()
    sum_copy.wait_recv()
    both = sum_send[...] + sum_recv[...]
    grad_conv = inv_std * (grad_normed - both[:, 0:1] / D - normed * (both[:, 1:2] / D))
    ext[pl.ds(0, 128), :] = grad_conv.astype(BF16).astype(F32)

    def reach_copy(to):
        return sp_copy(ext.at[pl.ds(0, 32)], ext.at[pl.ds(128, 32)], h_send, h_recv, to)

    @pl.when(me == 63)
    def _():
        ext[pl.ds(128, 32), :] = jnp.zeros((32, HALF), F32)

    @pl.when(me > 0)
    def _():
        reach_copy(me - 1).start()

    parts[pl.ds(here, 1)] = part[pl.ds(here, 1)]

    @pl.when(me < 63)
    def _():
        reach_copy(me + 1).wait_recv()

    def columns(c, _):
        cols = pl.ds(pl.multiple_of(c * 128, 128), 128)
        acc = jnp.zeros((128, 128), F32)
        for k in range(31):
            acc = acc + taps_f[pl.ds(k, 1), cols] * ext[pl.ds(k, 128), cols]
        gin_out[:, cols] = acc.astype(BF16)
        return 0

    lax.fori_loop(0, 8, columns, 0)

    def wait_part(d, _):
        part_arrived(lax.rem(here + d, 16)).wait_recv()
        return 0

    lax.fori_loop(1, 16, wait_part, 0)
    result = parts[0].astype(F32)
    for q in range(1, 16):
        result = result + parts[q].astype(F32)
    gproj_out[...] = result

    def sent_part(d, _):
        proj_copy(d).wait_send()
        return 0

    lax.fori_loop(1, 16, sent_part, 0)
    stream_copy(tp).wait_send()
    sum_copy.wait_send()
    for i in range(2):
        z = 2 * tp + i

        @pl.when(z != mz)
        def _():
            plane_copy(z, 0, i).wait_send()
            plane_copy(z, 1, i).wait_send()

    @pl.when(me > 0)
    def _():
        reach_copy(me - 1).wait_send()

    def finish_sends(i, _):
        @pl.when(i > 0)
        def _():
            direct_send(i).wait_send()

        twin_copy(i).wait_send()
        return 0

    lax.fori_loop(0, 32, finish_sends, 0)

    def finish(s, _):
        core_copy(s).wait_send()

        @pl.when(s != me)
        def _():
            ret_copy(s).wait_send()

        return 0

    lax.fori_loop(0, 64, finish, 0)
    for z in range(4):
        part_copy(z).wait_send()
    for _, _, sent in first_hop + second_hop + third_hop:
        sent()
    for d in (1, 2, 3):
        act_copy(d, True).wait_send()
    stat_copy.wait_send()
def store_kernel(*refs):
    sems = refs[10]
    copies = [pltpu.make_async_copy(refs[i], refs[5 + i], sems.at[i]) for i in range(5)]
    for copy in copies:
        copy.start()
    for copy in copies:
        copy.wait()


def on_device(
    conv_out, ln_gain, taps, proj_weight, stream_mid, out_grad,
    routes, route_probs, gate_slabs, up_slabs, down_slabs,
):
    hidden = gate_slabs.shape[2]
    rows = 768
    dma = pltpu.SemaphoreType.DMA
    vmem = pltpu.VMEM
    slots = vmem((64, 8, 1536), BF16)
    grad_input, grad_proj, grad_gate, grad_up, grad_down = pl.pallas_call(
        layer_kernel,
        out_shape=[
            jax.ShapeDtypeStruct((128, HALF), BF16),
            jax.ShapeDtypeStruct((32, HALF), F32),
            jax.ShapeDtypeStruct((D, hidden), BF16),
            jax.ShapeDtypeStruct((D, hidden), BF16),
            jax.ShapeDtypeStruct((hidden, D), BF16),
        ],
        in_specs=[pl.BlockSpec(memory_space=pl.ANY)] * 11,
        out_specs=[pl.BlockSpec(memory_space=pltpu.VMEM)] * 5,
        scratch_shapes=[
            vmem((2, 128), jnp.int32), vmem((2, 128), F32),
            vmem((128, HALF), BF16), vmem((128, HALF), BF16), vmem((128, HALF), BF16),
            vmem((1, HALF), F32), vmem((31, HALF), BF16),
            vmem((32, 8, 3072), BF16),
            vmem((64, 8, 3072), BF16), vmem((64, 8, 3072), BF16),
            vmem((rows, D), BF16), vmem((rows, D), BF16),
            vmem((rows, hidden), BF16), vmem((rows, hidden), BF16), vmem((rows, hidden), BF16),
            slots, slots, slots, slots,
            vmem((9, 256, 128), BF16), vmem((64, 128), BF16), vmem((64, 128), BF16),
            vmem((4, 4, 4, 32, HALF), BF16), vmem((4, 128, HALF), BF16),
            vmem((128, 128), F32), vmem((128, 128), F32), vmem((128, 128), F32),
            vmem((4, 128, 512), BF16), vmem((4, 128, 512), BF16),
            vmem((16, 32, HALF), BF16), vmem((16, 32, HALF), BF16),
            vmem((160, HALF), F32),
            vmem((128, 128), F32), vmem((128, 128), F32), vmem((32, HALF), F32),
            dma((4,)), dma((32,)), dma((32,)), dma((64,)), dma((64,)), dma((64,)),
            dma((4,)), dma((4,)), dma((64,)), dma((64,)),
            dma((8, 3)), dma((8, 3)), dma, dma, dma((3,)), dma((3,)),
            dma((7,)), dma, dma, dma((2, 2)), dma((4,)), dma((16,)), dma((16,)), dma, dma, dma, dma,
        ],
        compiler_params=pltpu.CompilerParams(
            collective_id=0, has_side_effects=True, vmem_limit_bytes=VMEM_BYTES
        ),
        name="layer",
    )(
        *(
            pltpu.with_memory_space_constraint(a, pltpu.HBM)
            for a in (
                routes.T, route_probs.T, stream_mid, out_grad, conv_out, ln_gain[None, :], taps,
                gate_slabs[0], up_slabs[0], down_slabs[0], proj_weight,
            )
        )
    )
    done = (grad_input, grad_proj, grad_gate, grad_up, grad_down)
    grad_input, grad_proj, grad_gate, grad_up, grad_down = pl.pallas_call(
        store_kernel,
        out_shape=[jax.ShapeDtypeStruct(a.shape, a.dtype) for a in done],
        in_specs=[pl.BlockSpec(memory_space=pltpu.VMEM)] * 5,
        out_specs=[pl.BlockSpec(memory_space=pl.ANY)] * 5,
        scratch_shapes=[dma((5,))],
        compiler_params=pltpu.CompilerParams(vmem_limit_bytes=1024 * 1024),
        name="store",
    )(*done)
    return grad_input, grad_proj, grad_gate[None], grad_up[None], grad_down[None]


def solution(mesh):
    return jax.shard_map(
        on_device,
        mesh=mesh,
        in_specs=(
            P("sp", "tp"), P("tp"), P(None, "tp"), P("sp", "tp"), P("sp", "tp"), P("sp", "tp"),
            P("sp", None), P("sp", None), P("sp", None, "tp"), P("sp", None, "tp"), P("sp", "tp", None),
        ),
        out_specs=(
            P("sp", "tp"), P("sp", "tp"), P("sp", None, "tp"), P("sp", None, "tp"), P("sp", "tp", None),
        ),
        check_vma=False,
    )
```

```python
import functools

import jax
import jax.numpy as jnp
from jax import lax
from jax.experimental import pallas as pl
from jax.experimental.pallas import tpu as pltpu
from jax.sharding import PartitionSpec as P

D = 2048
HALF = 1024
MAIN = 8
REM = 4
MESH = pl.DeviceIdType.MESH
F32 = jnp.float32
BF16 = jnp.bfloat16
VMEM_BYTES = 42 * 1024 * 1024


def nt(a, b):
    return lax.dot_general(a, b, (((1,), (1,)), ((), ())), preferred_element_type=F32)


def nn(a, b):
    return lax.dot_general(a, b, (((1,), (0,)), ((), ())), preferred_element_type=F32)


def tn(a, b):
    return lax.dot_general(a, b, (((0,), (0,)), ((), ())), preferred_element_type=F32)


def sp_copy(src, dst, send, recv, sp):
    return pltpu.make_async_remote_copy(
        src_ref=src, dst_ref=dst, send_sem=send, recv_sem=recv,
        device_id={"sp": sp}, device_id_type=MESH,
    )


def tp_copy(src, dst, send, recv, tp):
    return pltpu.make_async_remote_copy(
        src_ref=src, dst_ref=dst, send_sem=send, recv_sem=recv,
        device_id={"tp": tp}, device_id_type=MESH,
    )


def order(k):
    return lax.rem(k * 2, 4) + k // 2


def layer_kernel(
    routes_hbm, probs_hbm, stream_hbm, out_grad_hbm, conv_hbm, gain_hbm, taps_hbm,
    wg_hbm, wu_hbm, wd_hbm, proj_hbm,
    gin_out, gproj_out, wg, wu, wd,
    routes, probs, stream, out_grad, conv, gain, taps,
    pk, own, oth, xs, ps, acts, dgs, dus, psend, precv, pown, ret,
    table, sel_a, sel_b, proj, act, stat_send, stat_recv, stats,
    gs, gz, part, parts, ext, sum_send, sum_recv, taps_f,
    w_sem, a_send, b_send, c_send, own_sem, oth_sem,
    e_send, e_recv, r_send, r_recv,
    g_send, g_recv, s_send, s_recv, t_send, t_recv,
    i_sem, q_send, q_recv, z_send, z_recv, p_send, p_recv, u_send, u_recv, h_send, h_recv,
):
    me = lax.axis_index("sp")
    tp = lax.axis_index("tp")
    peer = 1 - tp
    mx, my, mz = lax.rem(me, 4), lax.rem(me // 4, 4), me // 16
    here = lax.rem(me, 16)
    twin = me + 1 - 2 * lax.rem(me, 2)
    loads = [
        pltpu.make_async_copy(src, dst, w_sem.at[i])
        for i, (src, dst) in enumerate(((wg_hbm, wg), (wu_hbm, wu), (wd_hbm, wd)))
    ]
    small = [
        pltpu.make_async_copy(src, dst, i_sem.at[i])
        for i, (src, dst) in enumerate(
            (
                (routes_hbm, routes), (probs_hbm, probs), (stream_hbm, stream),
                (out_grad_hbm, out_grad), (conv_hbm, conv), (gain_hbm, gain), (taps_hbm, taps),
            )
        )
    ]
    for copy in small:
        copy.start()
    proj_load = pltpu.make_async_copy(proj_hbm, proj.at[mz, my, mx], w_sem.at[3])
    proj_load.start()
    for copy in loads:
        copy.start()

    barrier = pltpu.get_barrier_semaphore()

    def greet(k, _):
        pl.semaphore_signal(
            barrier, inc=1, device_id={"sp": lax.rem(me + k, 64)}, device_id_type=MESH
        )
        return 0

    lax.fori_loop(1, 64, greet, 0)
    pl.semaphore_signal(barrier, inc=1, device_id={"tp": peer}, device_id_type=MESH)
    for d in (1, 2, 3):
        pl.semaphore_signal(
            barrier, inc=1, device_id={"sp": lax.rem(mz + d, 4) * 16 + here, "tp": peer},
            device_id_type=MESH,
        )

    for copy in small:
        copy.wait()

    expert = lax.broadcasted_iota(jnp.int32, (128, 128), 0)
    other = lax.broadcasted_iota(jnp.int32, (128, 128), 1)
    picks = [expert == routes[j : j + 1, :] for j in range(2)]
    counts = picks[0].astype(F32) + picks[1].astype(F32)
    before = nn(counts.astype(BF16), (expert < other).astype(F32).astype(BF16))
    at = lax.broadcasted_iota(jnp.int32, (256, 128), 0)
    for j in range(2):
        slot_row = jnp.sum(jnp.where(picks[j], before, 0.0), axis=0, keepdims=True)
        slot_row = slot_row.astype(jnp.int32)
        base = routes[j : j + 1, :] * MAIN + slot_row
        near = jnp.where(slot_row < MAIN, base, -1)
        far = jnp.where(slot_row < MAIN, -1, base)
        table[3 * j] = (at == near).astype(F32).astype(BF16)
        table[3 * j + 1] = (at + MAIN == far).astype(F32).astype(BF16)
        table[3 * j + 2] = (at + REM == far).astype(F32).astype(BF16)
    for i in range(3):
        table[6 + i] = table[i] + table[3 + i]
    shape = (32, 8, HALF)
    pk[:, :, :HALF] = nn(table[6], stream[...]).astype(BF16).reshape(shape)
    rest = nn(table[7], stream[:, :512]) + nn(table[8], stream[:, 512:])
    pk[:, :, 2 * HALF : 2 * HALF + 512] = rest.astype(BF16).reshape(32, 8, 512)
    p_main = table[0].astype(F32) * probs[0:1, :] + table[3].astype(F32) * probs[1:2, :]
    p_main = jnp.sum(p_main, axis=1, keepdims=True)
    near = nn(table[6], out_grad[...]) * p_main
    pk[:, :, HALF : 2 * HALF] = near.astype(BF16).reshape(shape)
    p_rest = (table[1] + table[2]).astype(F32) * probs[0:1, :]
    p_rest = p_rest + (table[4] + table[5]).astype(F32) * probs[1:2, :]
    p_rest = jnp.sum(p_rest, axis=1, keepdims=True)
    rest = nn(table[7], out_grad[:, :512]) + nn(table[8], out_grad[:, 512:])
    pk[:, :, 2 * HALF + 512 :] = (rest * p_rest).astype(BF16).reshape(32, 8, 512)

    proj_load.wait()

    pl.semaphore_wait(barrier, 67)

    def direct_send(i):
        k, j = i // 8, lax.rem(i, 8)
        dz, dy, side = order(k), order(j // 2), lax.rem(j, 2)
        x = mx + side * (3 - 2 * mx)
        to = lax.rem(mz + dz, 4) * 16 + lax.rem(my + dy, 4) * 4 + x
        return sp_copy(pk.at[to // 2], own.at[me], a_send.at[i], own_sem.at[me], to)

    def start_direct(i, _):
        direct_send(i).start()
        return 0


    def gather(group, axis, part):
        def at(d):
            z, y, x = mz, my, mx
            if axis == 0:
                z = lax.rem(mz + d, 4)
            elif axis == 1:
                y = lax.rem(my + d, 4)
            else:
                x = lax.rem(mx + d, 4)
            return z, y, x

        def copy(d, send):
            z, y, x = at(0) if send else at(4 - d)
            to_z, to_y, to_x = at(d)
            block = proj.at[part(z, y, x)]
            return sp_copy(
                block, block, g_send.at[group, d - 1], g_recv.at[group, d - 1],
                to_z * 16 + to_y * 4 + to_x,
            )

        def start():
            for d in (1, 3, 2):
                copy(d, True).start()

        def take():
            for d in (1, 3, 2):
                copy(d, False).wait_recv()

        def sent():
            for d in (1, 3, 2):
                copy(d, True).wait_send()

        return start, take, sent

    every = slice(None)
    low, mid_cols, high = pl.ds(0, 384), pl.ds(384, 512), pl.ds(896, 128)
    first_hop = (
        gather(0, 2, lambda z, y, x: (z, y, x, every, pl.ds(0, 896))),
        gather(1, 1, lambda z, y, x: (z, y, x, every, high)),
    )
    second_hop = (
        gather(2, 1, lambda z, y, x: (z, y, every, every, low)),
        gather(3, 0, lambda z, y, x: (z, y, every, every, mid_cols)),
        gather(4, 0, lambda z, y, x: (z, every, x, every, high)),
    )
    third_hop = (
        gather(5, 0, lambda z, y, x: (z, every, every, every, low)),
        gather(6, 1, lambda z, y, x: (every, y, every, every, mid_cols)),
        gather(7, 2, lambda z, y, x: (every, every, x, every, high)),
    )
    for start, _, _ in first_hop:
        start()
    lax.fori_loop(1, 32, start_direct, 0)

    row = lax.broadcasted_iota(jnp.int32, (64, 128), 0)
    col = lax.broadcasted_iota(jnp.int32, (64, 128), 1)
    spot = (row // 4) * 8 + row % 4
    sel_a[...] = (col == spot).astype(F32).astype(BF16)
    sel_b[...] = (col == spot + 4).astype(F32).astype(BF16)
    own[pl.ds(me, 1)] = pk[pl.ds(me // 2, 1)]
    values = conv[...].astype(F32)
    lane = lax.broadcasted_iota(jnp.int32, (128, 128), 1)
    total = jnp.sum(values, axis=1, keepdims=True)
    squares = jnp.sum(values * values, axis=1, keepdims=True)
    stat_send[...] = jnp.where(lane == 0, total, squares)
    stat_copy = tp_copy(stat_send, stat_recv, s_send, s_recv, peer)
    stat_copy.start()

    stat_copy.wait_recv()
    both = stat_send[...] + stat_recv[...]
    row_mean = both[:, 0:1] / D
    row_var = both[:, 1:2] / D - row_mean * row_mean
    inv_std = lax.rsqrt(row_var + 1e-06)
    stats[...] = jnp.where(lane == 0, row_mean, inv_std)
    scaled_z = (values - row_mean) * inv_std * gain[...]
    act[pl.ds(mz, 1)] = (scaled_z * jax.nn.sigmoid(scaled_z)).astype(BF16)[None]

    def act_copy(d, send):
        z = mz if send else lax.rem(mz + 4 - d, 4)
        return sp_copy(
            act.at[z], act.at[z], t_send.at[d - 1], t_recv.at[d - 1],
            lax.rem(mz + d, 4) * 16 + lax.rem(me, 16),
        )

    def source(k, j, near):
        dz, dy, side = order(k), order(j // 2), lax.rem(j, 2)
        x = mx + side * (3 - 2 * mx)
        twin_x = x + 1 - 2 * lax.rem(x, 2)
        x = x if near else twin_x
        return lax.rem(mz - dz + 4, 4) * 16 + lax.rem(my - dy + 4, 4) * 4 + x

    def twin_copy(i):
        s = source(i // 8, lax.rem(i, 8), True)
        return sp_copy(own.at[s], own.at[s], b_send.at[i], own_sem.at[s], twin)

    def core_copy(s):
        return tp_copy(own.at[s], oth.at[s], c_send.at[s], oth_sem.at[s], peer)

    def arrived(s):
        return sp_copy(own.at[s], own.at[s], c_send.at[s], own_sem.at[s], twin)

    def take_direct(k):
        def one(j, _):
            s = source(k, j, True)

            @pl.when(k * 8 + j != 0)
            def _():
                arrived(s).wait_recv()

            twin_copy(k * 8 + j).start()
            core_copy(s).start()
            return 0

        lax.fori_loop(0, 8, one, 0)

    def take_twin(k):
        def one(j, _):
            s = source(k, j, False)
            arrived(s).wait_recv()
            core_copy(s).start()
            return 0

        lax.fori_loop(0, 8, one, 0)

    def part_copy(z):
        return tp_copy(
            psend.at[pl.ds(z * 16, 16)], precv.at[pl.ds(z * 16, 16)],
            e_send.at[z], e_recv.at[z], peer,
        )

    def slot(s):
        return lax.rem(s, 2) * 32 + s // 2

    def ret_copy(s):
        return sp_copy(pown.at[s], ret.at[slot(me)], r_send.at[s], r_recv.at[me], s)

    def ret_arrived(s):
        return sp_copy(pown.at[s], ret.at[slot(s)], r_send.at[s], r_recv.at[s], s)

    def plane(k):
        return lax.rem(mz - order(k) + 4, 4)

    def compute(k):
        z = plane(k)

        def wait_other(j, _):
            tp_copy(
                own.at[z * 16 + j], oth.at[z * 16 + j],
                c_send.at[z * 16 + j], oth_sem.at[z * 16 + j], peer,
            ).wait_recv()
            return 0

        lax.fori_loop(0, 16, wait_other, 0)
        base = pl.multiple_of(z * 192, 64)
        for buf, half in ((own, tp), (oth, peer)):
            block = buf[pl.ds(z * 16, 16)].reshape(128, 3072)
            left = pl.multiple_of(half * HALF, HALF)
            mid = pl.multiple_of(half * HALF + 512, 512)
            xs[pl.ds(base, 128), pl.ds(left, HALF)] = block[:, :HALF]
            ps[pl.ds(base, 128), pl.ds(left, HALF)] = block[:, HALF : 2 * HALF]
            rest = block[:, 2 * HALF :]
            first = nn(sel_a[...], rest).astype(BF16)
            second = nn(sel_b[...], rest).astype(BF16)
            low = pl.multiple_of(base + 128, 64)
            xs[pl.ds(low, 64), pl.ds(left, 512)] = first[:, :512]
            xs[pl.ds(low, 64), pl.ds(mid, 512)] = second[:, :512]
            ps[pl.ds(low, 64), pl.ds(left, 512)] = first[:, 512:]
            ps[pl.ds(low, 64), pl.ds(mid, 512)] = second[:, 512:]
        x = xs[pl.ds(base, 192), :]
        p = ps[pl.ds(base, 192), :]
        g = nn(x, wg[...])
        u = nn(x, wu[...])
        dh = nt(p, wd[...])
        sig = jax.nn.sigmoid(g)
        silu = g * sig
        acts[pl.ds(base, 192), :] = (silu * u).astype(BF16)
        dg = (dh * u * sig * (1.0 + g * (1.0 - sig))).astype(BF16)
        du = (dh * silu).astype(BF16)
        dgs[pl.ds(base, 192), :] = dg
        dus[pl.ds(base, 192), :] = du
        for out, half in ((psend, peer), (pown, tp)):
            rows = pl.ds(pl.multiple_of(half * HALF, HALF), HALF)
            back = nt(dg, wg[rows, :]) + nt(du, wu[rows, :])
            back = back.astype(BF16)
            out[pl.ds(z * 16, 16), :, :HALF] = back[:128].reshape(16, 8, HALF)
            rest = tn(sel_a[...], back[128:, :512]) + tn(sel_b[...], back[128:, 512:])
            out[pl.ds(z * 16, 16), :, HALF:] = rest.astype(BF16).reshape(16, 8, 512)
            if half is peer:
                part_copy(z).start()

    def give_back(k):
        z = plane(k)
        part_copy(z).wait_recv()
        block = pl.ds(z * 16, 16)
        pown[block] = (pown[block].astype(F32) + precv[block].astype(F32)).astype(BF16)

        def one(j, _):
            s = z * 16 + lax.rem(lax.rem(me, 16) + j, 16)

            @pl.when(s != me)
            def _():
                ret_copy(s).start()

            return 0

        lax.fori_loop(0, 16, one, 0)

    for _, take, _ in first_hop:
        take()
    for start, _, _ in second_hop:
        start()
    take_direct(0)
    for d in (1, 3, 2):
        act_copy(d, True).start()
    take_direct(1)
    for _, take, _ in second_hop:
        take()
    for start, _, _ in third_hop[:2]:
        start()
    take_twin(0)
    for copy in loads:
        copy.wait()

    def step(k, _):
        @pl.when(k < 2)
        def _():
            take_direct(k + 2)

        @pl.when(k > 0)
        def _():
            give_back(k - 1)

        compute(k)

        @pl.when(k < 3)
        def _():
            take_twin(k + 1)


        return 0

    lax.fori_loop(0, 4, step, 0)
    give_back(3)
    ret[pl.ds(slot(me), 1)] = pown[pl.ds(me, 1)]
    third_hop[2][0]()

    def weight_grads(i, _):
        cols = pl.ds(pl.multiple_of(i * 256, 256), 256)
        rows = xs[:, cols].T
        wg[cols, :] = nn(rows, dgs[...]).astype(BF16)
        wu[cols, :] = nn(rows, dus[...]).astype(BF16)
        return 0

    lax.fori_loop(0, 8, weight_grads, 0)

    def down_grads(i, _):
        cols = pl.ds(pl.multiple_of(i * 128, 128), 128)
        wd[cols, :] = nn(acts[:, cols].T, ps[...]).astype(BF16)
        return 0

    lax.fori_loop(0, 7, down_grads, 0)
    taps_f[pl.ds(0, 31), :] = taps[...].astype(F32)

    def await_return(s, _):
        @pl.when(s != me)
        def _():
            ret_arrived(s).wait_recv()

        return 0

    lax.fori_loop(0, 64, await_return, 0)
    contrib = jnp.zeros((128, HALF), F32)
    halves = []
    for h in range(2):
        block = ret[pl.ds(h * 32, 32)].reshape(256, 1536)
        contrib = contrib + tn(table[6], block[:, :HALF])
        halves.append(block[:, HALF:])
    left = tn(table[7], halves[0]) + tn(table[7], halves[1])
    right = tn(table[8], halves[0]) + tn(table[8], halves[1])
    left = (out_grad[:, :512].astype(F32) + (contrib[:, :512] + left)).astype(BF16)
    right = (out_grad[:, 512:].astype(F32) + (contrib[:, 512:] + right)).astype(BF16)
    gs[pl.ds(2 * tp, 1)] = left[None]
    gs[pl.ds(2 * tp + 1, 1)] = right[None]

    def stream_copy(tp_of):
        rows = pl.ds(2 * tp_of, 2)
        return tp_copy(gs.at[rows], gs.at[rows], q_send, q_recv, peer)

    def plane_copy(z, core, i):
        return pltpu.make_async_remote_copy(
            src_ref=gs.at[z], dst_ref=gz.at[mz],
            send_sem=z_send.at[i, core], recv_sem=z_recv.at[mz],
            device_id={"sp": z * 16 + here, "tp": core}, device_id_type=MESH,
        )

    def plane_arrived(z):
        return sp_copy(gz.at[z], gz.at[z], z_send.at[0, 0], z_recv.at[z], z * 16 + here)

    stream_copy(tp).start()
    for i in range(2):
        z = 2 * tp + i

        @pl.when(z != mz)
        def _():
            plane_copy(z, 0, i).start()
            plane_copy(z, 1, i).start()

    for d in (1, 2, 3):
        act_copy(d, False).wait_recv()

    def weights(z):
        return proj[pl.ds(z, 1)].reshape(512, HALF)

    for _, take, _ in third_hop:
        take()
    grad_act = nn(left, weights(2 * tp)) + nn(right, weights(2 * tp + 1))
    stream_copy(peer).wait_recv()
    mine = gs[pl.ds(mz, 1)].reshape(128, 512)
    total = tn(mine, act[pl.ds(mz, 1)].reshape(128, HALF))
    for d in (1, 3, 2):
        z = lax.rem(mz + d, 4)
        plane_arrived(z).wait_recv()
        total = total + tn(gz[pl.ds(z, 1)].reshape(128, 512), act[pl.ds(z, 1)].reshape(128, HALF))
    part[...] = total.astype(BF16).reshape(16, 32, HALF)

    def proj_copy(d):
        q = lax.rem(here + d, 16)
        return sp_copy(part.at[q], parts.at[here], p_send.at[d], p_recv.at[here], mz * 16 + q)

    def part_arrived(q):
        return sp_copy(parts.at[q], parts.at[q], p_send.at[0], p_recv.at[q], mz * 16 + q)

    def start_part(d, _):
        proj_copy(d).start()
        return 0

    other = gs[pl.ds(2 * peer, 2)]
    grad_act = grad_act + nn(other[0], weights(2 * peer)) + nn(other[1], weights(2 * peer + 1))
    lax.fori_loop(1, 16, start_part, 0)

    row_mean, inv_std = stats[:, 0:1], stats[:, 1:2]
    normed = (conv[...].astype(F32) - row_mean) * inv_std
    scaled_z = normed * gain[...]
    z_sig = jax.nn.sigmoid(scaled_z)
    grad_normed = grad_act * z_sig * (1.0 + scaled_z * (1.0 - z_sig)) * gain[...]
    sum_send[...] = jnp.where(
        lane == 0,
        jnp.sum(grad_normed, axis=1, keepdims=True),
        jnp.sum(grad_normed * normed, axis=1, keepdims=True),
    )
    sum_copy = tp_copy(sum_send, sum_recv, u_send, u_recv, peer)
    sum_copy.start()
    sum_copy.wait_recv()
    both = sum_send[...] + sum_recv[...]
    grad_conv = inv_std * (grad_normed - both[:, 0:1] / D - normed * (both[:, 1:2] / D))
    ext[pl.ds(0, 128), :] = grad_conv.astype(BF16).astype(F32)

    def reach_copy(to):
        return sp_copy(ext.at[pl.ds(0, 32)], ext.at[pl.ds(128, 32)], h_send, h_recv, to)

    @pl.when(me == 63)
    def _():
        ext[pl.ds(128, 32), :] = jnp.zeros((32, HALF), F32)

    @pl.when(me > 0)
    def _():
        reach_copy(me - 1).start()

    parts[pl.ds(here, 1)] = part[pl.ds(here, 1)]

    @pl.when(me < 63)
    def _():
        reach_copy(me + 1).wait_recv()

    def columns(c, _):
        cols = pl.ds(pl.multiple_of(c * 128, 128), 128)
        acc = jnp.zeros((128, 128), F32)
        for k in range(31):
            acc = acc + taps_f[pl.ds(k, 1), cols] * ext[pl.ds(k, 128), cols]
        gin_out[:, cols] = acc.astype(BF16)
        return 0

    lax.fori_loop(0, 8, columns, 0)

    def wait_part(d, _):
        part_arrived(lax.rem(here + d, 16)).wait_recv()
        return 0

    lax.fori_loop(1, 16, wait_part, 0)
    result = parts[0].astype(F32)
    for q in range(1, 16):
        result = result + parts[q].astype(F32)
    gproj_out[...] = result

    def sent_part(d, _):
        proj_copy(d).wait_send()
        return 0

    lax.fori_loop(1, 16, sent_part, 0)
    stream_copy(tp).wait_send()
    sum_copy.wait_send()
    for i in range(2):
        z = 2 * tp + i

        @pl.when(z != mz)
        def _():
            plane_copy(z, 0, i).wait_send()
            plane_copy(z, 1, i).wait_send()

    @pl.when(me > 0)
    def _():
        reach_copy(me - 1).wait_send()

    def finish_sends(i, _):
        @pl.when(i > 0)
        def _():
            direct_send(i).wait_send()

        twin_copy(i).wait_send()
        return 0

    lax.fori_loop(0, 32, finish_sends, 0)

    def finish(s, _):
        core_copy(s).wait_send()

        @pl.when(s != me)
        def _():
            ret_copy(s).wait_send()

        return 0

    lax.fori_loop(0, 64, finish, 0)
    for z in range(4):
        part_copy(z).wait_send()
    for _, _, sent in first_hop + second_hop + third_hop:
        sent()
    for d in (1, 2, 3):
        act_copy(d, True).wait_send()
    stat_copy.wait_send()
def store_kernel(*refs):
    sems = refs[10]
    copies = [pltpu.make_async_copy(refs[i], refs[5 + i], sems.at[i]) for i in range(5)]
    for copy in copies:
        copy.start()
    for copy in copies:
        copy.wait()


def on_device(
    conv_out, ln_gain, taps, proj_weight, stream_mid, out_grad,
    routes, route_probs, gate_slabs, up_slabs, down_slabs,
):
    hidden = gate_slabs.shape[2]
    rows = 768
    dma = pltpu.SemaphoreType.DMA
    vmem = pltpu.VMEM
    slots = vmem((64, 8, 1536), BF16)
    grad_input, grad_proj, grad_gate, grad_up, grad_down = pl.pallas_call(
        layer_kernel,
        out_shape=[
            jax.ShapeDtypeStruct((128, HALF), BF16),
            jax.ShapeDtypeStruct((32, HALF), F32),
            jax.ShapeDtypeStruct((D, hidden), BF16),
            jax.ShapeDtypeStruct((D, hidden), BF16),
            jax.ShapeDtypeStruct((hidden, D), BF16),
        ],
        in_specs=[pl.BlockSpec(memory_space=pl.ANY)] * 11,
        out_specs=[pl.BlockSpec(memory_space=pltpu.VMEM)] * 5,
        scratch_shapes=[
            vmem((2, 128), jnp.int32), vmem((2, 128), F32),
            vmem((128, HALF), BF16), vmem((128, HALF), BF16), vmem((128, HALF), BF16),
            vmem((1, HALF), F32), vmem((31, HALF), BF16),
            vmem((32, 8, 3072), BF16),
            vmem((64, 8, 3072), BF16), vmem((64, 8, 3072), BF16),
            vmem((rows, D), BF16), vmem((rows, D), BF16),
            vmem((rows, hidden), BF16), vmem((rows, hidden), BF16), vmem((rows, hidden), BF16),
            slots, slots, slots, slots,
            vmem((9, 256, 128), BF16), vmem((64, 128), BF16), vmem((64, 128), BF16),
            vmem((4, 4, 4, 32, HALF), BF16), vmem((4, 128, HALF), BF16),
            vmem((128, 128), F32), vmem((128, 128), F32), vmem((128, 128), F32),
            vmem((4, 128, 512), BF16), vmem((4, 128, 512), BF16),
            vmem((16, 32, HALF), BF16), vmem((16, 32, HALF), BF16),
            vmem((160, HALF), F32),
            vmem((128, 128), F32), vmem((128, 128), F32), vmem((32, HALF), F32),
            dma((4,)), dma((32,)), dma((32,)), dma((64,)), dma((64,)), dma((64,)),
            dma((4,)), dma((4,)), dma((64,)), dma((64,)),
            dma((8, 3)), dma((8, 3)), dma, dma, dma((3,)), dma((3,)),
            dma((7,)), dma, dma, dma((2, 2)), dma((4,)), dma((16,)), dma((16,)), dma, dma, dma, dma,
        ],
        compiler_params=pltpu.CompilerParams(
            collective_id=0, has_side_effects=True, vmem_limit_bytes=VMEM_BYTES
        ),
        name="layer",
    )(
        *(
            pltpu.with_memory_space_constraint(a, pltpu.HBM)
            for a in (
                routes.T, route_probs.T, stream_mid, out_grad, conv_out, ln_gain[None, :], taps,
                gate_slabs[0], up_slabs[0], down_slabs[0], proj_weight,
            )
        )
    )
    done = (grad_input, grad_proj, grad_gate, grad_up, grad_down)
    grad_input, grad_proj, grad_gate, grad_up, grad_down = pl.pallas_call(
        store_kernel,
        out_shape=[jax.ShapeDtypeStruct(a.shape, a.dtype) for a in done],
        in_specs=[pl.BlockSpec(memory_space=pltpu.VMEM)] * 5,
        out_specs=[pl.BlockSpec(memory_space=pl.ANY)] * 5,
        scratch_shapes=[dma((5,))],
        compiler_params=pltpu.CompilerParams(vmem_limit_bytes=1024 * 1024),
        name="store",
    )(*done)
    return grad_input, grad_proj, grad_gate[None], grad_up[None], grad_down[None]


def solution(mesh):
    return jax.shard_map(
        on_device,
        mesh=mesh,
        in_specs=(
            P("sp", "tp"), P("tp"), P(None, "tp"), P("sp", "tp"), P("sp", "tp"), P("sp", "tp"),
            P("sp", None), P("sp", None), P("sp", None, "tp"), P("sp", None, "tp"), P("sp", "tp", None),
        ),
        out_specs=(
            P("sp", "tp"), P("sp", "tp"), P("sp", None, "tp"), P("sp", None, "tp"), P("sp", "tp", None),
        ),
        check_vma=False,
    )
```
